256 devices in a mesh: grp: 2 (over y), sp: 32 (over z, core), tp: 4 (over x).
Axes of the slice: x: 4, y: 2, z: 16, core: 2. Of those that a mesh axis runs over, the one named last changes fastest.
The devices are a block of a 4x16x16 slice.
Arguments:
- residual: bfloat16 [32768, 2048], P(('grp', 'sp', 'tp')), parts along dimension 0, may hold values from -6 to 6
- state_input: bfloat16 [32768, 1024], P(('grp', 'sp'), 'tp'), parts along dimension 0, may hold values from -6 to 6
- gate_input: bfloat16 [32768, 2048], P(('grp', 'sp'), 'tp'), parts along dimension 0, may hold values from -6 to 6
- decay_real: float32 [64, 64], P('tp'), may hold values from -0.2 to 0, as said below
- frequency: float32 [64, 64], P('tp'), as said below
- log_step: float32 [64], P('tp'), as said below
- drive_real: float32 [64, 64, 16], P('tp'), may hold values from -1 to 1
- drive_imag: float32 [64, 64, 16], P('tp'), may hold values from -1 to 1
- read_real: float32 [64, 16, 64], P('tp'), may hold values from -0.75 to 0.75
- read_imag: float32 [64, 16, 64], P('tp'), may hold values from -0.75 to 0.75
- skip_gain: float32 [1024], P('tp'), may hold values from -4 to 4
- value_weight: bfloat16 [1024, 2048], P(None, 'tp'), may hold values from -0.1875 to 0.1875
- glu_weight: bfloat16 [1024, 2048], P(None, 'tp'), may hold values from -0.1875 to 0.1875
- mix_weight: bfloat16 [2048, 2048], P('tp'), may hold values from -0.125 to 0.125
- norm_gain: float32 [2048], replicated, may hold values from 0.1 to 1.9
- mlp_gate: bfloat16 [2048, 3072], P('sp', 'tp'), may hold values from -0.125 to 0.125
- mlp_up: bfloat16 [2048, 3072], P('sp', 'tp'), may hold values from -0.125 to 0.125
- mlp_down: bfloat16 [3072, 2048], P('tp', 'sp'), may hold values from -0.109375 to 0.109375
Outputs:
- result: bfloat16 [32768, 2048], P(('grp', 'sp', 'tp')), parts along dimension 0
The draws below stay inside these ranges and needn't reach their ends.
There are 2 independent parts, one for each index of `grp`. The reference program is written for one: setup_inputs(seed, part) draws one part's arguments, and reference() takes and returns one part's arrays. A program takes and returns all parts, laid end to end along the dimension named above; an argument that names none is the same for every part. Nothing has to cross between parts.
Inputs may be any that keep to these rules, and one draw needn't show every extreme that they name: `decay_real`: negative in every entry. `frequency`: never zero: its magnitude times exp(log_step) of its group lies between 0.05 and 0.5. Every group's time step exp(log_step) is at most one.
All inputs are finite; a program needn't handle non-finite values.
Results may differ from the reference program's by a relative error of at most 0.012.
Values may be sent and summed in bfloat16 or wider, within the bound.
No kernel may reach another device: no remote copies, remote signals or barrier semaphores. Data moves between devices by JAX's collectives and lax.ppermute only.
A program may use at most 128 MiB of HBM per device.

```python
import math
import jax
import jax.numpy as jnp
from jax import lax

D = 2048
D_SSM = 1024
SSM_GROUP = 16
STATE = 64
FF = 3072
TOK_DEV = 512
GROUPS = 64
TOKENS = 16384
N_TP = 4


def spectrum(key):
    fast_key = jax.random.fold_in(key, 101)
    rate_key = jax.random.fold_in(key, 202)
    spread_key = jax.random.fold_in(key, 303)
    turn_key = jax.random.fold_in(key, 404)
    sign_key = jax.random.fold_in(key, 505)
    share = 0.5
    fast = jax.random.uniform(fast_key, (GROUPS,), jnp.float32) < share
    unit = jax.random.uniform(rate_key, (GROUPS,), jnp.float32)
    fast_rate = jnp.exp(math.log(1.0 / 40.0) + unit * math.log(2.0))
    slow_rate = jnp.exp(jnp.log(0.5 / TOKENS) + unit * math.log(4.0))
    rate = jnp.where(fast, fast_rate, slow_rate)
    step = 2.0 * jnp.sqrt(rate)
    spread = jnp.exp(jax.random.uniform(spread_key, (GROUPS, STATE), jnp.float32, math.log(0.7), math.log(1.4)))
    decay = -(rate / step)[:, None] * spread
    turn = jax.random.uniform(turn_key, (GROUPS, STATE), jnp.float32, 0.05, 0.5)
    sign = jnp.where(jax.random.uniform(sign_key, (GROUPS, STATE), jnp.float32) < 0.5, -1.0, 1.0)
    frequency = sign * turn / step[:, None]
    return (decay, frequency, jnp.log(step))


def draw_decay_real(key, part):
    return spectrum(key)[0]


def draw_frequency(key, part):
    return spectrum(key)[1]


def draw_log_step(key, part):
    return spectrum(key)[2]


def block_scale(rng, extent, cuts, smallest, top_value):
    factor_of, own = 1.0, jax.random.fold_in(rng, 6)
    for axis_at, blocks in cuts:
        steps = jnp.exp(jax.random.uniform(jax.random.fold_in(own, axis_at), (blocks,), jnp.float32, smallest / len(cuts), top_value / len(cuts)))
        factor_of = factor_of * jnp.repeat(steps, extent[axis_at] // blocks).reshape([-1 if axis == axis_at else 1 for axis in range(len(extent))])
    return factor_of


def bell_draw(key, dims, scale, bound, split=(), dtype=jnp.bfloat16):
    drawn = scale * jax.random.normal(key, dims, jnp.float32)
    if split:
        drawn = drawn * block_scale(key, dims, split, -0.22, 0.18)
    return jnp.clip(drawn, -bound, bound).astype(dtype)


def setup_inputs(seed: int = 0, part: int = 0) -> dict:
    keys = jax.random.split(jax.random.key(seed), 19)
    part_splits = jax.random.split(jax.random.fold_in(keys[18], part), 19)
    residual = bell_draw(part_splits[0], (TOKENS, D), 1.0, 6.0, ((0, 128),))
    state_input = bell_draw(part_splits[1], (TOKENS, D_SSM), 1.0, 6.0, ((0, 32), (1, 4)))
    gate_input = bell_draw(part_splits[2], (TOKENS, D), 1.5, 6.0, ((0, 32), (1, 4)))
    decay_real = draw_decay_real(jax.random.fold_in(keys[18], 71), part)
    frequency = draw_frequency(jax.random.fold_in(keys[18], 71), part)
    log_step = draw_log_step(jax.random.fold_in(keys[18], 71), part)
    drive_real = bell_draw(keys[6], (GROUPS, STATE, SSM_GROUP), (2 * SSM_GROUP) ** -0.5, 1.0, ((0, 4),), jnp.float32)
    drive_imag = bell_draw(keys[7], (GROUPS, STATE, SSM_GROUP), (2 * SSM_GROUP) ** -0.5, 1.0, ((0, 4),), jnp.float32)
    read_real = bell_draw(keys[8], (GROUPS, SSM_GROUP, STATE), STATE ** -0.5, 0.75, ((0, 4),), jnp.float32)
    read_imag = bell_draw(keys[9], (GROUPS, SSM_GROUP, STATE), STATE ** -0.5, 0.75, ((0, 4),), jnp.float32)
    skip_gain = bell_draw(keys[10], (D_SSM,), 1.0, 4.0, ((0, 4),), jnp.float32)
    value_weight = bell_draw(keys[11], (D_SSM, D), D_SSM ** -0.5, 0.1875, ((1, 4),))
    glu_weight = bell_draw(keys[12], (D_SSM, D), D_SSM ** -0.5, 0.1875, ((1, 4),))
    mix_weight = bell_draw(keys[13], (D, D), D ** -0.5, 0.125, ((0, 4),))
    norm_gain = jnp.clip(1.0 + 0.18 * jax.random.normal(keys[14], (D,), jnp.float32), 0.1, 1.9)
    mlp_gate = bell_draw(keys[15], (D, FF), D ** -0.5, 0.125, ((0, 32), (1, 4)))
    mlp_up = bell_draw(keys[16], (D, FF), D ** -0.5, 0.125, ((0, 32), (1, 4)))
    mlp_down = bell_draw(keys[17], (FF, D), FF ** -0.5, 0.109375, ((0, 4), (1, 32)))
    return {"residual": residual, "state_input": state_input, "gate_input": gate_input, "decay_real": decay_real, "frequency": frequency, "log_step": log_step, "drive_real": drive_real, "drive_imag": drive_imag, "read_real": read_real, "read_imag": read_imag, "skip_gain": skip_gain, "value_weight": value_weight, "glu_weight": glu_weight, "mix_weight": mix_weight, "norm_gain": norm_gain, "mlp_gate": mlp_gate, "mlp_up": mlp_up, "mlp_down": mlp_down}


HIGH = lax.Precision.HIGHEST
EPSILON = 1e-06

def discretize(decay_real, frequency, log_step, drive_real, drive_imag):
    step = jnp.exp(log_step)[:, None]
    magnitude = jnp.exp(decay_real * step)
    turned = frequency * step
    bar_real = magnitude * jnp.cos(turned)
    bar_imag = magnitude * jnp.sin(turned)
    modulus = decay_real * decay_real + frequency * frequency
    ratio_real = ((bar_real - 1.0) * decay_real + bar_imag * frequency) / modulus
    ratio_imag = (bar_imag * decay_real - (bar_real - 1.0) * frequency) / modulus
    in_real = ratio_real[..., None] * drive_real - ratio_imag[..., None] * drive_imag
    in_imag = ratio_real[..., None] * drive_imag + ratio_imag[..., None] * drive_real
    return (bar_real, bar_imag, in_real, in_imag)

def combine(earlier, later):
    real_one, imag_one, state_real_one, state_imag_one = earlier
    real_two, imag_two, state_real_two, state_imag_two = later
    return (real_one * real_two - imag_one * imag_two, real_one * imag_two + imag_one * real_two, real_two * state_real_one - imag_two * state_imag_one + state_real_two, real_two * state_imag_one + imag_two * state_real_one + state_imag_two)

def block_states(inputs, bar_real, bar_imag, in_real, in_imag):
    rows = inputs.shape[0]
    flat = bar_real.shape[0] * bar_real.shape[1]
    push_real = jnp.einsum('lgh,gph->lgp', inputs, in_real, precision=HIGH).reshape(rows, flat)
    push_imag = jnp.einsum('lgh,gph->lgp', inputs, in_imag, precision=HIGH).reshape(rows, flat)
    power_real = jnp.broadcast_to(bar_real.reshape(1, flat), (rows, flat))
    power_imag = jnp.broadcast_to(bar_imag.reshape(1, flat), (rows, flat))
    return lax.associative_scan(combine, (power_real, power_imag, push_real, push_imag), axis=0)

def readout(state_real, state_imag, read_real, read_imag, inputs, skip_gain):
    rows = inputs.shape[0]
    groups, width, states = read_real.shape
    grid_real = state_real.reshape(rows, groups, states)
    grid_imag = state_imag.reshape(rows, groups, states)
    output = jnp.einsum('lgp,ghp->lgh', grid_real, read_real, precision=HIGH)
    output = output - jnp.einsum('lgp,ghp->lgh', grid_imag, read_imag, precision=HIGH)
    output = output.reshape(rows, groups * width) + skip_gain * inputs.reshape(rows, groups * width)
    return jax.nn.gelu(output).astype(jnp.bfloat16)

def normalize(inner, norm_gain):
    scale = lax.rsqrt(lax.optimization_barrier(jnp.mean(inner * inner, axis=-1, keepdims=True)) + EPSILON)
    return (inner * scale * norm_gain).astype(jnp.bfloat16)

def reference(residual, state_input, gate_input, decay_real, frequency, log_step, drive_real, drive_imag, read_real, read_imag, skip_gain, value_weight, glu_weight, mix_weight, norm_gain, mlp_gate, mlp_up, mlp_down):
    bar_real, bar_imag, in_real, in_imag = discretize(decay_real, frequency, log_step, drive_real, drive_imag)
    groups, states = bar_real.shape
    blocks = state_input.astype(jnp.float32).reshape(TOKENS // TOK_DEV, TOK_DEV, groups, SSM_GROUP)

    def advance(carry, inputs):
        carry_real, carry_imag = carry
        power_real, power_imag, local_real, local_imag = block_states(inputs, bar_real, bar_imag, in_real, in_imag)
        state_real = local_real + power_real * carry_real - power_imag * carry_imag
        state_imag = local_imag + power_real * carry_imag + power_imag * carry_real
        acts = readout(state_real, state_imag, read_real, read_imag, inputs, skip_gain)
        return ((state_real[-1], state_imag[-1]), acts)
    zero = jnp.zeros((groups * states,), jnp.float32)
    _, acts = lax.scan(advance, (zero, zero), blocks)
    acts = acts.reshape(TOKENS, D_SSM)
    value = jnp.dot(acts, value_weight, preferred_element_type=jnp.float32)
    gated = jnp.dot(acts, glu_weight, preferred_element_type=jnp.float32)
    mixed = (jax.nn.sigmoid(gate_input.astype(jnp.float32)) * value * jax.nn.sigmoid(gated)).astype(jnp.bfloat16)
    span = D // N_TP
    branch = jnp.zeros((TOKENS, D), jnp.float32)
    for index in range(N_TP):
        product = jnp.dot(mixed[:, index * span:(index + 1) * span], mix_weight[index * span:(index + 1) * span], preferred_element_type=jnp.float32).astype(jnp.bfloat16)
        branch = branch + lax.optimization_barrier(product).astype(jnp.float32)
    inner = residual.astype(jnp.float32) + branch
    normed = normalize(inner, norm_gain)
    hidden_gate = jnp.dot(normed, mlp_gate, preferred_element_type=jnp.float32)
    hidden_up = jnp.dot(normed, mlp_up, preferred_element_type=jnp.float32)
    hidden = (jax.nn.silu(hidden_gate) * hidden_up).astype(jnp.bfloat16)
    width = FF // N_TP
    down = jnp.zeros((TOKENS, D), jnp.float32)
    for index in range(N_TP):
        product = jnp.dot(hidden[:, index * width:(index + 1) * width], mlp_down[index * width:(index + 1) * width], preferred_element_type=jnp.float32).astype(jnp.bfloat16)
        down = down + lax.optimization_barrier(product).astype(jnp.float32)
    return (inner + 0.5 * down).astype(jnp.bfloat16)
```

```python
import functools

import jax
import jax.numpy as jnp
from jax import lax
from jax.experimental import pallas as pl
from jax.experimental.pallas import tpu as pltpu
from jax.sharding import PartitionSpec as P

EPSILON = 1e-06
SEGMENTS = 8
LANES = 128
F32 = jnp.float32
BF16 = jnp.bfloat16
NT = (((1,), (1,)), ((), ()))


def times(a, b):
    return a[0] * b[0] - a[1] * b[1], a[0] * b[1] + a[1] * b[0]


def plus(a, b):
    return a[0] + b[0], a[1] + b[1]


def squared(a, count):
    for _ in range(count):
        a = times(a, a)
    return a


def iota(shape, dim):
    return lax.broadcasted_iota(jnp.int32, shape, dim)


def bits(size):
    assert size & (size - 1) == 0
    return size.bit_length() - 1


def along_lanes(x, count):
    while x.shape[1] % 128 and count > 1:
        x, count = jnp.concatenate([x, x], axis=1), count // 2
    return jnp.concatenate([x] * count, axis=1) if count > 1 else x


def as_row(x):
    groups, states = x.shape
    wide = along_lanes(x, groups)
    own = iota(wide.shape, 1) >> bits(states) == iota(wide.shape, 0)
    return jnp.sum(jnp.where(own, wide, 0.0), axis=0, keepdims=True)


def rates(decay_ref, freq_ref, log_step_ref):
    decay, freq = decay_ref[...], freq_ref[...]
    groups = decay.shape[0]
    wide = jnp.broadcast_to(log_step_ref[...], (groups, groups))
    same = iota(wide.shape, 0) == iota(wide.shape, 1)
    step = jnp.exp(jnp.sum(jnp.where(same, wide, 0.0), axis=1, keepdims=True))
    size = jnp.exp(decay * step)
    x = freq * step
    q = x * x
    cos = 1.0 + q * (-1 / 2 + q * (1 / 24 + q * (-1 / 720 + q * (1 / 40320 - q / 3628800))))
    sin = x * (1.0 + q * (-1 / 6 + q * (1 / 120 + q * (-1 / 5040 + q / 362880))))
    bar = size * cos, size * sin
    modulus = decay * decay + freq * freq
    ratio = (
        ((bar[0] - 1.0) * decay + bar[1] * freq) / modulus,
        (bar[1] * decay - (bar[0] - 1.0) * freq) / modulus,
    )
    return (as_row(bar[0]), as_row(bar[1])), (as_row(ratio[0]), as_row(ratio[1]))


def fill_drive(x_ref, b_re_ref, b_im_ref, xf_ref, xp_ref, d_re_ref, d_im_ref):
    rows, chans = x_ref.shape
    flat, width = b_re_ref.shape
    states = flat * width // chans
    length = rows // SEGMENTS
    for i in range(chans // LANES):
        at = slice(i * LANES, (i + 1) * LANES)
        xf_ref[i] = x_ref[:, at].astype(F32)
        for j in range(length):
            xp_ref[j * SEGMENTS : (j + 1) * SEGMENTS, at] = xf_ref[
                i, pl.ds(j, SEGMENTS, stride=length), :
            ]
    x = xp_ref[...].astype(BF16)
    shape = (flat, chans)
    pick = (iota((width, chans), 1) & (width - 1) == iota((width, chans), 0)).astype(BF16)
    own = iota(shape, 0) >> bits(states) == iota(shape, 1) >> bits(width)
    for b_ref, d_ref in ((b_re_ref, d_re_ref), (b_im_ref, d_im_ref)):
        wide = jnp.dot(b_ref[...].astype(BF16), pick, preferred_element_type=F32)
        wide = jnp.where(own, wide, 0.0).astype(BF16)
        d_ref[...] = lax.dot_general(x, wide, NT, preferred_element_type=F32)


def wide_read(c_re_ref, c_im_ref, factor):
    chans, states = c_re_ref.shape
    flat = factor[0].shape[1]
    groups = flat // states
    width = chans // groups
    shape = (chans, flat)
    own = iota(shape, 0) >> bits(width) == iota(shape, 1) >> bits(states)
    c = along_lanes(c_re_ref[...], groups), along_lanes(c_im_ref[...], groups)
    re, im = times(c, factor)
    return jnp.concatenate(
        [jnp.where(own, re, 0.0).astype(BF16), jnp.where(own, -im, 0.0).astype(BF16)], axis=1
    )


def ends_kernel(
    decay_ref, freq_ref, log_step_ref, x_ref, b_re_ref, b_im_ref,
    end_ref, seg_ref, row_ref, near_ref, far_ref,
    xf_ref, xp_ref, d_re_ref, d_im_ref,
):
    rows, flat = d_re_ref.shape
    length = rows // SEGMENTS
    bar, ratio = rates(decay_ref, freq_ref, log_step_ref)
    fill_drive(x_ref, b_re_ref, b_im_ref, xf_ref, xp_ref, d_re_ref, d_im_ref)
    lam = tuple(jnp.broadcast_to(part, (SEGMENTS, flat)) for part in bar)

    def advance(j, state):
        at = pl.ds(pl.multiple_of(j * SEGMENTS, SEGMENTS), SEGMENTS)
        return plus(times(lam, state), (d_re_ref[at, :], d_im_ref[at, :]))

    zero = jnp.zeros((SEGMENTS, flat), F32)
    ends = lax.fori_loop(0, length, advance, (zero, zero), unroll=4)
    over = squared(bar, bits(length))
    carry = jnp.zeros((1, flat), F32), jnp.zeros((1, flat), F32)
    for s in range(SEGMENTS):
        seg_ref[0, s : s + 1, :], seg_ref[1, s : s + 1, :] = carry
        carry = plus(times(over, carry), tuple(part[s : s + 1, :] for part in ends))
    end_ref[0:1, :], end_ref[1:2, :] = carry
    for i, part in enumerate((*bar, *ratio)):
        row_ref[i : i + 1, :] = part
    block = squared(over, bits(SEGMENTS))
    one = jnp.ones((1, flat), F32), jnp.zeros((1, flat), F32)
    for ref in (near_ref, far_ref):
        power = one
        for k in range(ref.shape[1]):
            ref[0, k : k + 1, :], ref[1, k : k + 1, :] = power
            power = times(power, block)
        block = power


def local_kernel(
    row_ref, seg_ref, x_ref, b_re_ref, b_im_ref, c_re_ref, c_im_ref, skip_ref,
    y_ref, power_ref,
    xf_ref, xp_ref, d_re_ref, d_im_ref, s_ref, w_ref,
):
    rows, flat = d_re_ref.shape
    length = rows // SEGMENTS
    fill_drive(x_ref, b_re_ref, b_im_ref, xf_ref, xp_ref, d_re_ref, d_im_ref)
    bar = row_ref[0:1, :], row_ref[1:2, :]
    ratio = row_ref[2:3, :], row_ref[3:4, :]
    lam = tuple(jnp.broadcast_to(part, (SEGMENTS, flat)) for part in bar)

    def advance(j, state):
        at = pl.ds(pl.multiple_of(j * 2 * SEGMENTS, 2 * SEGMENTS), 2 * SEGMENTS)
        d_re, d_im = d_re_ref[at, :], d_im_ref[at, :]
        first = plus(times(lam, state), (d_re[:SEGMENTS], d_im[:SEGMENTS]))
        second = plus(times(lam, first), (d_re[SEGMENTS:], d_im[SEGMENTS:]))
        for i in (0, 1):
            both = jnp.concatenate([first[i], second[i]], axis=0)
            s_ref[at, i * flat : (i + 1) * flat] = both.astype(BF16)
        return second

    lax.fori_loop(0, length // 2, advance, (seg_ref[0], seg_ref[1]), unroll=2)
    over = squared(bar, bits(length))
    power = jnp.ones((1, flat), F32), jnp.zeros((1, flat), F32)
    for s in range(SEGMENTS):
        w_ref[0, s : s + 1, :], w_ref[1, s : s + 1, :] = power
        power = times(power, over)

    def raise_power(j, power):
        at = pl.ds(pl.multiple_of(j * 2 * SEGMENTS, 2 * SEGMENTS), 2 * SEGMENTS)
        first = times(lam, power)
        second = times(lam, first)
        for i in (0, 1):
            both = jnp.concatenate([first[i], second[i]], axis=0)
            power_ref[at, i * flat : (i + 1) * flat] = both.astype(BF16)
        return second

    lax.fori_loop(0, length // 2, raise_power, (w_ref[0], w_ref[1]), unroll=2)
    read = wide_read(c_re_ref, c_im_ref, ratio)
    out = lax.dot_general(s_ref[...], read, NT, preferred_element_type=F32)
    y_ref[...] = out + skip_ref[...] * xp_ref[...]


def sum_kernel(count, *refs):
    pieces, pow_ref, out_ref = refs[:count], refs[count], refs[count + 1]
    total = None
    for k, ref in enumerate(pieces):
        piece = ref[0:1, :], ref[1:2, :]
        if k:
            piece = times((pow_ref[0, k : k + 1, :], pow_ref[1, k : k + 1, :]), piece)
        total = piece if total is None else plus(total, piece)
    out_ref[0:1, :], out_ref[1:2, :] = total


def finish_kernel(count, *refs):
    pieces = refs[:count]
    pow_ref, row_ref, c_re_ref, c_im_ref, y_ref, power_ref, out_ref, t_ref = refs[count:]
    total = None
    for k, ref in enumerate(pieces):
        piece = ref[0:1, :], ref[1:2, :]
        if k:
            piece = times((pow_ref[0, k : k + 1, :], pow_ref[1, k : k + 1, :]), piece)
        total = piece if total is None else plus(total, piece)
    ratio = row_ref[2:3, :], row_ref[3:4, :]
    read = wide_read(c_re_ref, c_im_ref, times(ratio, total))
    y = y_ref[...] + lax.dot_general(power_ref[...], read, NT, preferred_element_type=F32)
    y = jax.nn.gelu(y, approximate=True)
    length = y.shape[0] // SEGMENTS
    for i in range(y.shape[1] // LANES):
        at = slice(i * LANES, (i + 1) * LANES)
        for j in range(length):
            t_ref[i, pl.ds(j, SEGMENTS, stride=length), :] = y[
                j * SEGMENTS : (j + 1) * SEGMENTS, at
            ]
        out_ref[:, at] = t_ref[i].astype(BF16)


def shaped(*shape, dtype=F32):
    return jax.ShapeDtypeStruct(shape, dtype)


def shifted(array, axis, by):
    peers = lax.axis_size(axis)
    return lax.ppermute(array, axis, [(i, i + by) for i in range(peers - by)])


def activations(
    state_input, decay_real, frequency, log_step, drive_real, drive_imag,
    read_real, read_imag, skip_gain,
):
    rows, chans = state_input.shape
    groups, states = decay_real.shape
    width = chans // groups
    flat = groups * states
    peers = lax.axis_size("sp")
    near = 1
    while near * near < peers:
        near += 1
    far = -(-peers // near)
    log_row = log_step.reshape(1, groups)
    b = [part.reshape(flat, width) for part in (drive_real, drive_imag)]
    c = [part.reshape(chans, states) for part in (read_real, read_imag)]
    skip = skip_gain.reshape(1, chans)
    drive_scratch = [
        pltpu.VMEM((chans // LANES, rows, LANES), F32),
        pltpu.VMEM((rows, chans), F32),
        pltpu.VMEM((rows, flat), F32),
        pltpu.VMEM((rows, flat), F32),
    ]
    end, seg, row, near_powers, far_powers = pl.pallas_call(
        ends_kernel,
        out_shape=(
            shaped(2, flat),
            shaped(2, SEGMENTS, flat),
            shaped(4, flat),
            shaped(2, near, flat),
            shaped(2, far, flat),
        ),
        scratch_shapes=drive_scratch,
        name="ssm_ends",
    )(decay_real, frequency, log_row, state_input, *b)
    first = [shifted(end, "sp", k + 1) for k in range(near)]
    local, power = pl.pallas_call(
        local_kernel,
        out_shape=(shaped(rows, chans), shaped(rows, 2 * flat, dtype=BF16)),
        scratch_shapes=[
            *drive_scratch,
            pltpu.VMEM((rows, 2 * flat), BF16),
            pltpu.VMEM((2, SEGMENTS, flat), F32),
        ],
        cost_estimate=pl.CostEstimate(
            flops=8 * rows * flat * chans, bytes_accessed=8 * rows * flat, transcendentals=0
        ),
        name="ssm_local",
    )(row, seg, state_input, *b, *c, skip)
    joined = pl.pallas_call(
        functools.partial(sum_kernel, near), out_shape=shaped(2, flat), name="ssm_join"
    )(*first, near_powers)
    second = [joined] + [shifted(joined, "sp", k * near) for k in range(1, far)]
    return pl.pallas_call(
        functools.partial(finish_kernel, far),
        out_shape=shaped(rows, chans, dtype=BF16),
        scratch_shapes=[pltpu.VMEM((chans // LANES, rows, LANES), F32)],
        name="ssm_finish",
    )(*second, far_powers, row, *c, local, power)


def ring(array, by):
    peers = lax.axis_size("tp")
    return lax.ppermute(array, "tp", [(i, (i + by) % peers) for i in range(peers)])


def rows_at(array, index, size):
    return lax.dynamic_slice_in_dim(array, index * size, size, 0)


def gathered(own):
    half = own.shape[0] // 2
    top, low = own[:half], own[half:]
    left_top, right_low = ring(top, 1), ring(low, -1)
    left_low, right_top = ring(low, 1), ring(top, -1)
    far_top, far_low = ring(left_top, 1), ring(right_low, -1)
    return (top, low), (left_top, left_low), (right_top, right_low), (far_top, far_low)


def summed(product, me, peers):
    far = product((me + 2) % peers).astype(BF16)
    half = far.shape[0] // 2
    from_left, from_right = ring(far[:half], 1), ring(far[half:], -1)
    right = product((me + 1) % peers)
    left = product((me + 3) % peers)
    in_low = ring(right[half:].astype(BF16), 1)
    in_top = ring(left[:half].astype(BF16), -1)
    in_top_left = ring((right[:half] + from_left.astype(F32)).astype(BF16), 1)
    in_low_right = ring((left[half:] + from_right.astype(F32)).astype(BF16), -1)
    own = product(me)
    top = own[:half] + in_top.astype(F32) + in_top_left.astype(F32)
    low = own[half:] + in_low.astype(F32) + in_low_right.astype(F32)
    return jnp.concatenate([top, low], axis=0)


def shards(
    residual, state_input, gate_input, decay_real, frequency, log_step,
    drive_real, drive_imag, read_real, read_imag, skip_gain,
    value_weight, glu_weight, mix_weight, norm_gain, mlp_gate, mlp_up, mlp_down,
):
    peers, me = lax.axis_size("tp"), lax.axis_index("tp")
    assert peers == 4
    hidden_width = mlp_gate.shape[1]
    both = jnp.concatenate([mlp_gate, mlp_up], axis=1)
    both = lax.all_gather(both, "sp", axis=0, tiled=True)
    down_weight = lax.all_gather(mlp_down.T, "sp", axis=0, tiled=True)

    acts = activations(
        state_input, decay_real, frequency, log_step, drive_real, drive_imag,
        read_real, read_imag, skip_gain,
    )
    chans = acts.shape[1]
    order = [me, (me + 3) % peers, (me + 1) % peers, (me + 2) % peers]
    in_weight = jnp.concatenate(
        [
            jnp.concatenate([rows_at(w, q, chans) for q in order], axis=0)
            for w in (value_weight, glu_weight)
        ],
        axis=1,
    )
    width = value_weight.shape[1]
    pieces = gathered(acts)
    piece = jnp.concatenate([jnp.concatenate(pair, axis=0) for pair in pieces], axis=1)
    value = jnp.dot(piece, in_weight[:, :width], preferred_element_type=F32)
    gated = jnp.dot(piece, in_weight[:, width:], preferred_element_type=F32)
    mixed = (jax.nn.sigmoid(gate_input.astype(F32)) * value * jax.nn.sigmoid(gated)).astype(BF16)

    owned = residual.shape[0]
    branch = summed(
        lambda q: jnp.dot(rows_at(mixed, q, owned), mix_weight, preferred_element_type=F32),
        me, peers,
    )
    inner = residual.astype(F32) + branch
    scale = lax.rsqrt(jnp.mean(inner * inner, axis=-1, keepdims=True) + EPSILON)
    normed = (inner * scale * norm_gain).astype(BF16)
    places = dict(zip((0, 3, 1, 2), gathered(normed)))

    def down_product(q):
        return products[q]

    def feed(pair):
        rows = jnp.concatenate(pair, axis=0)
        hidden = jnp.dot(rows, both, preferred_element_type=F32)
        hidden = (jax.nn.silu(hidden[:, :hidden_width]) * hidden[:, hidden_width:]).astype(BF16)
        return lax.dot_general(hidden, down_weight, NT, preferred_element_type=F32)

    products = {place: feed(pair) for place, pair in places.items()}
    down = summed(lambda q: products[q], 0, peers)
    return (inner + 0.5 * down).astype(BF16)


def solution(mesh):
    placed = (
        P(("grp", "sp", "tp"), None),
        P(("grp", "sp"), "tp"),
        P(("grp", "sp"), "tp"),
        P("tp", None),
        P("tp", None),
        P("tp"),
        P("tp", None, None),
        P("tp", None, None),
        P("tp", None, None),
        P("tp", None, None),
        P("tp"),
        P(None, "tp"),
        P(None, "tp"),
        P("tp", None),
        P(),
        P("sp", "tp"),
        P("sp", "tp"),
        P("tp", "sp"),
    )
    return jax.shard_map(
        shards, mesh=mesh, in_specs=placed, out_specs=P(("grp", "sp", "tp"), None), check_vma=False
    )
```

```python
import jax
import jax.numpy as jnp
from jax import lax
from jax.experimental import pallas as pl
from jax.experimental.pallas import tpu as pltpu
from jax.sharding import PartitionSpec as P

EPSILON = 1e-06
SEGMENTS = 8
LANES = 128
F32 = jnp.float32
BF16 = jnp.bfloat16
NT = (((1,), (1,)), ((), ()))


def times(a, b):
    return a[0] * b[0] - a[1] * b[1], a[0] * b[1] + a[1] * b[0]


def plus(a, b):
    return a[0] + b[0], a[1] + b[1]


def squared(a, count):
    for _ in range(count):
        a = times(a, a)
    return a


def iota(shape, dim):
    return lax.broadcasted_iota(jnp.int32, shape, dim)


def bits(size):
    assert size & (size - 1) == 0
    return size.bit_length() - 1


def along_lanes(x, count):
    while x.shape[1] % 128 and count > 1:
        x, count = jnp.concatenate([x, x], axis=1), count // 2
    return jnp.concatenate([x] * count, axis=1) if count > 1 else x


def as_row(x):
    groups, states = x.shape
    wide = along_lanes(x, groups)
    own = iota(wide.shape, 1) >> bits(states) == iota(wide.shape, 0)
    return jnp.sum(jnp.where(own, wide, 0.0), axis=0, keepdims=True)


def rates(decay_ref, freq_ref, log_step_ref):
    decay, freq = decay_ref[...], freq_ref[...]
    groups = decay.shape[0]
    wide = jnp.broadcast_to(log_step_ref[...], (groups, groups))
    same = iota(wide.shape, 0) == iota(wide.shape, 1)
    step = jnp.exp(jnp.sum(jnp.where(same, wide, 0.0), axis=1, keepdims=True))
    size = jnp.exp(decay * step)
    x = freq * step
    q = x * x
    cos = 1.0 + q * (-1 / 2 + q * (1 / 24 + q * (-1 / 720 + q * (1 / 40320 - q / 3628800))))
    sin = x * (1.0 + q * (-1 / 6 + q * (1 / 120 + q * (-1 / 5040 + q / 362880))))
    bar = size * cos, size * sin
    modulus = decay * decay + freq * freq
    ratio = (
        ((bar[0] - 1.0) * decay + bar[1] * freq) / modulus,
        (bar[1] * decay - (bar[0] - 1.0) * freq) / modulus,
    )
    return (as_row(bar[0]), as_row(bar[1])), (as_row(ratio[0]), as_row(ratio[1]))


def fill_drive(x_ref, b_re_ref, b_im_ref, xf_ref, xp_ref, d_re_ref, d_im_ref):
    rows, chans = x_ref.shape
    states = b_re_ref.shape[1]
    flat = d_re_ref.shape[1]
    groups = flat // states
    length = rows // SEGMENTS
    for i in range(chans // LANES):
        at = slice(i * LANES, (i + 1) * LANES)
        xf_ref[i] = x_ref[:, at].astype(F32)

        def permute(j, _, i=i, at=at):
            to = pl.ds(pl.multiple_of(j * SEGMENTS, SEGMENTS), SEGMENTS)
            xp_ref[to, at] = xf_ref[i, pl.ds(j, SEGMENTS, stride=length), :]
            return 0

        lax.fori_loop(0, length, permute, 0, unroll=8)
    x = xp_ref[...].astype(BF16)
    shape = (chans, flat)
    own = iota(shape, 0) >> bits(chans // groups) == iota(shape, 1) >> bits(states)
    for b_ref, d_ref in ((b_re_ref, d_re_ref), (b_im_ref, d_im_ref)):
        wide = jnp.where(own, along_lanes(b_ref[...], groups), 0.0).astype(BF16)
        d_ref[...] = jnp.dot(x, wide, preferred_element_type=F32)


def wide_read(c_re_ref, c_im_ref, factor):
    chans, states = c_re_ref.shape
    flat = factor[0].shape[1]
    groups = flat // states
    width = chans // groups
    shape = (chans, flat)
    own = iota(shape, 0) >> bits(width) == iota(shape, 1) >> bits(states)
    c = along_lanes(c_re_ref[...], groups), along_lanes(c_im_ref[...], groups)
    re, im = times(c, factor)
    return jnp.concatenate(
        [jnp.where(own, re, 0.0).astype(BF16), jnp.where(own, -im, 0.0).astype(BF16)], axis=1
    )


def as_tile(row):
    return jnp.concatenate(
        [row[:, i : i + LANES] for i in range(0, row.shape[1], LANES)], axis=0
    )


def from_tile(tile):
    return jnp.concatenate([tile[i : i + 1, :] for i in range(tile.shape[0])], axis=1)


def ends_kernel(
    me_ref, decay_ref, freq_ref, log_step_ref, x_ref, b_re_ref, b_im_ref,
    gate_ref, up_ref, down_ref,
    end_ref, seg_ref, row_ref, weight_ref,
    xf_ref, xp_ref, d_re_ref, d_im_ref,
):
    rows, flat = d_re_ref.shape
    length = rows // SEGMENTS
    at = 0
    for ref in (gate_ref, up_ref, down_ref):
        weight_ref[:, at : at + ref.shape[1]] = ref[...]
        at += ref.shape[1]
    bar, ratio = rates(decay_ref, freq_ref, log_step_ref)
    fill_drive(x_ref, b_re_ref, b_im_ref, xf_ref, xp_ref, d_re_ref, d_im_ref)
    lam = tuple(jnp.broadcast_to(part, (SEGMENTS, flat)) for part in bar)

    def advance(j, state):
        at = pl.ds(pl.multiple_of(j * SEGMENTS, SEGMENTS), SEGMENTS)
        return plus(times(lam, state), (d_re_ref[at, :], d_im_ref[at, :]))

    zero = jnp.zeros((SEGMENTS, flat), F32)
    ends = lax.fori_loop(0, length, advance, (zero, zero), unroll=4)
    over = squared(bar, bits(length))
    carry = jnp.zeros((1, flat), F32), jnp.zeros((1, flat), F32)
    for s in range(SEGMENTS):
        seg_ref[0, s : s + 1, :], seg_ref[1, s : s + 1, :] = carry
        carry = plus(times(over, carry), tuple(part[s : s + 1, :] for part in ends))
    for i, part in enumerate((*bar, *ratio)):
        row_ref[i : i + 1, :] = part
    block = tuple(as_tile(part) for part in squared(over, bits(SEGMENTS)))
    state = tuple(as_tile(part) for part in carry)
    me = me_ref[0]
    for place in range(end_ref.shape[0]):
        later = place > me
        sent = jnp.concatenate(state, axis=0)
        end_ref[place] = jnp.where(later, sent, 0.0).astype(BF16)
        state = tuple(
            jnp.where(later, new, old) for new, old in zip(times(block, state), state)
        )


def local_kernel(
    row_ref, seg_ref, x_ref, b_re_ref, b_im_ref, c_re_ref, c_im_ref, skip_ref,
    y_ref, power_ref,
    xf_ref, xp_ref, d_re_ref, d_im_ref, s_ref, w_ref,
):
    rows, flat = d_re_ref.shape
    length = rows // SEGMENTS
    fill_drive(x_ref, b_re_ref, b_im_ref, xf_ref, xp_ref, d_re_ref, d_im_ref)
    bar = row_ref[0:1, :], row_ref[1:2, :]
    ratio = row_ref[2:3, :], row_ref[3:4, :]
    lam = tuple(jnp.broadcast_to(part, (SEGMENTS, flat)) for part in bar)

    def advance(j, state):
        at = pl.ds(pl.multiple_of(j * 2 * SEGMENTS, 2 * SEGMENTS), 2 * SEGMENTS)
        d_re, d_im = d_re_ref[at, :], d_im_ref[at, :]
        first = plus(times(lam, state), (d_re[:SEGMENTS], d_im[:SEGMENTS]))
        second = plus(times(lam, first), (d_re[SEGMENTS:], d_im[SEGMENTS:]))
        for i in (0, 1):
            both = jnp.concatenate([first[i], second[i]], axis=0)
            s_ref[at, i * flat : (i + 1) * flat] = both.astype(BF16)
        return second

    lax.fori_loop(0, length // 2, advance, (seg_ref[0], seg_ref[1]), unroll=2)
    over = squared(bar, bits(length))
    power = jnp.ones((1, flat), F32), jnp.zeros((1, flat), F32)
    for s in range(SEGMENTS):
        w_ref[0, s : s + 1, :], w_ref[1, s : s + 1, :] = power
        power = times(power, over)

    def raise_power(j, power):
        at = pl.ds(pl.multiple_of(j * 2 * SEGMENTS, 2 * SEGMENTS), 2 * SEGMENTS)
        first = times(lam, power)
        second = times(lam, first)
        for i in (0, 1):
            both = jnp.concatenate([first[i], second[i]], axis=0)
            power_ref[at, i * flat : (i + 1) * flat] = both.astype(BF16)
        return second

    lax.fori_loop(0, length // 2, raise_power, (w_ref[0], w_ref[1]), unroll=2)
    read = wide_read(c_re_ref, c_im_ref, ratio)
    out = lax.dot_general(s_ref[...], read, NT, preferred_element_type=F32)
    y_ref[...] = out + skip_ref[...] * xp_ref[...]


def finish_kernel(
    piece_ref, row_ref, c_re_ref, c_im_ref, y_ref, power_ref, out_ref, t_ref
):
    pieces = jnp.sum(piece_ref[...].astype(F32), axis=0)
    half = pieces.shape[0] // 2
    total = from_tile(pieces[:half]), from_tile(pieces[half:])
    ratio = row_ref[2:3, :], row_ref[3:4, :]
    read = wide_read(c_re_ref, c_im_ref, times(ratio, total))
    y = y_ref[...] + lax.dot_general(power_ref[...], read, NT, preferred_element_type=F32)
    y = jax.nn.gelu(y, approximate=True)
    length = y.shape[0] // SEGMENTS
    for i in range(y.shape[1] // LANES):
        at = slice(i * LANES, (i + 1) * LANES)
        for j in range(length):
            t_ref[i, pl.ds(j, SEGMENTS, stride=length), :] = y[
                j * SEGMENTS : (j + 1) * SEGMENTS, at
            ]
        out_ref[:, at] = t_ref[i].astype(BF16)


def shaped(*shape, dtype=F32):
    return jax.ShapeDtypeStruct(shape, dtype)


def activations(
    state_input, decay_real, frequency, log_step, drive_real, drive_imag,
    read_real, read_imag, skip_gain, weights,
):
    rows, chans = state_input.shape
    groups, states = decay_real.shape
    flat = groups * states
    peers = lax.axis_size("sp")
    me = lax.axis_index("sp").reshape(1)
    log_row = log_step.reshape(1, groups)
    b = [part.transpose(0, 2, 1).reshape(chans, states) for part in (drive_real, drive_imag)]
    c = [part.reshape(chans, states) for part in (read_real, read_imag)]
    skip = skip_gain.reshape(1, chans)
    drive_scratch = [
        pltpu.VMEM((chans // LANES, rows, LANES), F32),
        pltpu.VMEM((rows, chans), F32),
        pltpu.VMEM((rows, flat), F32),
        pltpu.VMEM((rows, flat), F32),
    ]
    whole = pl.BlockSpec(memory_space=pltpu.VMEM)
    end, seg, row, weight = pl.pallas_call(
        ends_kernel,
        out_shape=(
            shaped(peers, 2 * flat // LANES, LANES, dtype=BF16),
            shaped(2, SEGMENTS, flat),
            shaped(4, flat),
            shaped(weights[0].shape[0], sum(w.shape[1] for w in weights), dtype=BF16),
        ),
        in_specs=[pl.BlockSpec(memory_space=pltpu.SMEM), *[whole] * 9],
        scratch_shapes=drive_scratch,
        name="ssm_ends",
    )(me, decay_real, frequency, log_row, state_input, *b, *weights)
    weight = lax.all_gather(weight, "sp", axis=0, tiled=True)
    pieces = lax.all_to_all(end, "sp", 0, 0, tiled=True)
    local, power = pl.pallas_call(
        local_kernel,
        out_shape=(shaped(rows, chans), shaped(rows, 2 * flat, dtype=BF16)),
        scratch_shapes=[
            *drive_scratch,
            pltpu.VMEM((rows, 2 * flat), BF16),
            pltpu.VMEM((2, SEGMENTS, flat), F32),
        ],
        cost_estimate=pl.CostEstimate(
            flops=8 * rows * flat * chans, bytes_accessed=8 * rows * flat, transcendentals=0
        ),
        name="ssm_local",
    )(row, seg, state_input, *b, *c, skip)
    acts = pl.pallas_call(
        finish_kernel,
        out_shape=shaped(rows, chans, dtype=BF16),
        scratch_shapes=[pltpu.VMEM((chans // LANES, rows, LANES), F32)],
        name="ssm_finish",
    )(pieces, row, *c, local, power)
    return acts, weight


def ring(array, by):
    peers = lax.axis_size("tp")
    return lax.ppermute(array, "tp", [(i, (i + by) % peers) for i in range(peers)])


def rows_at(array, index, size):
    return lax.dynamic_slice_in_dim(array, index * size, size, 0)


def gathered(own):
    half = own.shape[0] // 2
    left = ring(own, 1)
    right = ring(own, -1)
    far_top = ring(left[:half], 1)
    far_low = ring(right[half:], -1)
    return own, left, right, jnp.concatenate([far_top, far_low], axis=0)


def summed(product, me, peers):
    far = product((me + 2) % peers).astype(BF16)
    half = far.shape[0] // 2
    from_left, from_right = ring(far[:half], 1), ring(far[half:], -1)
    right = product((me + 1) % peers)
    left = product((me + 3) % peers)
    right = right + jnp.pad(from_left, ((0, half), (0, 0))).astype(F32)
    left = left + jnp.pad(from_right, ((half, 0), (0, 0))).astype(F32)
    from_left, from_right = ring(right.astype(BF16), 1), ring(left.astype(BF16), -1)
    return product(me) + from_left.astype(F32) + from_right.astype(F32)


def shards(
    residual, state_input, gate_input, decay_real, frequency, log_step,
    drive_real, drive_imag, read_real, read_imag, skip_gain,
    value_weight, glu_weight, mix_weight, norm_gain, mlp_gate, mlp_up, mlp_down,
):
    peers, me = lax.axis_size("tp"), lax.axis_index("tp")
    assert peers == 4
    hidden_width = mlp_gate.shape[1]
    chans = state_input.shape[1]
    acts, weight = activations(
        state_input, decay_real, frequency, log_step, drive_real, drive_imag,
        read_real, read_imag, skip_gain, (mlp_gate, mlp_up, mlp_down.T),
    )
    both, down_weight = weight[:, : 2 * hidden_width], weight[:, 2 * hidden_width :]
    places = dict(zip((0, 3, 1, 2), (acts, ring(acts, 1), ring(acts, -1), ring(acts, 2))))

    def project(w):
        total = None
        for place, rows in places.items():
            part = jnp.dot(
                rows, rows_at(w, (me + place) % peers, chans), preferred_element_type=F32
            )
            total = part if total is None else total + part
        return total

    value, gated = project(value_weight), project(glu_weight)
    mixed = (jax.nn.sigmoid(gate_input.astype(F32)) * value * jax.nn.sigmoid(gated)).astype(BF16)

    owned = residual.shape[0]
    branch = summed(
        lambda q: jnp.dot(rows_at(mixed, q, owned), mix_weight, preferred_element_type=F32),
        me, peers,
    )
    inner = residual.astype(F32) + branch
    scale = lax.rsqrt(jnp.mean(inner * inner, axis=-1, keepdims=True) + EPSILON)
    normed = (inner * scale * norm_gain).astype(BF16)
    own, left, right, far = gathered(normed)

    def feed(rows):
        hidden = jnp.dot(rows, both, preferred_element_type=F32)
        hidden = (jax.nn.silu(hidden[:, :hidden_width]) * hidden[:, hidden_width:]).astype(BF16)
        return lax.dot_general(hidden, down_weight, NT, preferred_element_type=F32)

    near = feed(own)
    sides = feed(jnp.concatenate([left, right], axis=0))
    products = {0: near, 1: sides[owned:], 2: feed(far), 3: sides[:owned]}
    down = summed(lambda q: products[q], 0, peers)
    return (inner + 0.5 * down).astype(BF16)


def solution(mesh):
    placed = (
        P(("grp", "sp", "tp"), None),
        P(("grp", "sp"), "tp"),
        P(("grp", "sp"), "tp"),
        P("tp", None),
        P("tp", None),
        P("tp"),
        P("tp", None, None),
        P("tp", None, None),
        P("tp", None, None),
        P("tp", None, None),
        P("tp"),
        P(None, "tp"),
        P(None, "tp"),
        P("tp", None),
        P(),
        P("sp", "tp"),
        P("sp", "tp"),
        P("tp", "sp"),
    )

    return jax.shard_map(
        shards, mesh=mesh, in_specs=placed, out_specs=P(("grp", "sp", "tp"), None), check_vma=False
    )
```

```python
import jax
import jax.numpy as jnp
from jax import lax
from jax.experimental import pallas as pl
from jax.experimental.pallas import tpu as pltpu
from jax.sharding import PartitionSpec as P

EPSILON = 1e-06
SEGMENTS = 8
LANES = 128
F32 = jnp.float32
BF16 = jnp.bfloat16
NT = (((1,), (1,)), ((), ()))


def times(a, b):
    return a[0] * b[0] - a[1] * b[1], a[0] * b[1] + a[1] * b[0]


def plus(a, b):
    return a[0] + b[0], a[1] + b[1]


def squared(a, count):
    for _ in range(count):
        a = times(a, a)
    return a


def iota(shape, dim):
    return lax.broadcasted_iota(jnp.int32, shape, dim)


def bits(size):
    assert size & (size - 1) == 0
    return size.bit_length() - 1


def along_lanes(x, count):
    while x.shape[1] % 128 and count > 1:
        x, count = jnp.concatenate([x, x], axis=1), count // 2
    return jnp.concatenate([x] * count, axis=1) if count > 1 else x


def as_row(x):
    groups, states = x.shape
    wide = along_lanes(x, groups)
    own = iota(wide.shape, 1) >> bits(states) == iota(wide.shape, 0)
    return jnp.sum(jnp.where(own, wide, 0.0), axis=0, keepdims=True)


def rates(decay_ref, freq_ref, log_step_ref):
    decay, freq = decay_ref[...], freq_ref[...]
    groups = decay.shape[0]
    wide = jnp.broadcast_to(log_step_ref[...], (groups, groups))
    same = iota(wide.shape, 0) == iota(wide.shape, 1)
    step = jnp.exp(jnp.sum(jnp.where(same, wide, 0.0), axis=1, keepdims=True))
    size = jnp.exp(decay * step)
    x = freq * step
    q = x * x
    cos = 1.0 + q * (-1 / 2 + q * (1 / 24 + q * (-1 / 720 + q * (1 / 40320 - q / 3628800))))
    sin = x * (1.0 + q * (-1 / 6 + q * (1 / 120 + q * (-1 / 5040 + q / 362880))))
    bar = size * cos, size * sin
    modulus = decay * decay + freq * freq
    ratio = (
        ((bar[0] - 1.0) * decay + bar[1] * freq) / modulus,
        (bar[1] * decay - (bar[0] - 1.0) * freq) / modulus,
    )
    return (as_row(bar[0]), as_row(bar[1])), (as_row(ratio[0]), as_row(ratio[1]))


def fill_drive(x_ref, b_re_ref, b_im_ref, xf_ref, xp_ref, d_re_ref, d_im_ref):
    rows, chans = x_ref.shape
    states = b_re_ref.shape[1]
    flat = d_re_ref.shape[1]
    groups = flat // states
    length = rows // SEGMENTS
    for i in range(chans // LANES):
        at = slice(i * LANES, (i + 1) * LANES)
        xf_ref[i] = x_ref[:, at].astype(F32)

        def permute(j, _, i=i, at=at):
            to = pl.ds(pl.multiple_of(j * SEGMENTS, SEGMENTS), SEGMENTS)
            xp_ref[to, at] = xf_ref[i, pl.ds(j, SEGMENTS, stride=length), :]
            return 0

        lax.fori_loop(0, length, permute, 0, unroll=8)
    x = xp_ref[...].astype(BF16)
    shape = (chans, flat)
    own = iota(shape, 0) >> bits(chans // groups) == iota(shape, 1) >> bits(states)
    for b_ref, d_ref in ((b_re_ref, d_re_ref), (b_im_ref, d_im_ref)):
        wide = jnp.where(own, along_lanes(b_ref[...], groups), 0.0).astype(BF16)
        d_ref[...] = jnp.dot(x, wide, preferred_element_type=F32)


def wide_read(c_re_ref, c_im_ref, factor):
    chans, states = c_re_ref.shape
    flat = factor[0].shape[1]
    groups = flat // states
    width = chans // groups
    shape = (chans, flat)
    own = iota(shape, 0) >> bits(width) == iota(shape, 1) >> bits(states)
    c = along_lanes(c_re_ref[...], groups), along_lanes(c_im_ref[...], groups)
    re, im = times(c, factor)
    return jnp.concatenate(
        [jnp.where(own, re, 0.0).astype(BF16), jnp.where(own, -im, 0.0).astype(BF16)], axis=1
    )


def as_tile(row):
    return jnp.concatenate(
        [row[:, i : i + LANES] for i in range(0, row.shape[1], LANES)], axis=0
    )


def from_tile(tile):
    return jnp.concatenate([tile[i : i + 1, :] for i in range(tile.shape[0])], axis=1)


def ends_kernel(
    me_ref, decay_ref, freq_ref, log_step_ref, x_ref, b_re_ref, b_im_ref,
    gate_ref, up_ref, down_ref,
    end_ref, seg_ref, row_ref, weight_ref,
    xf_ref, xp_ref, d_re_ref, d_im_ref,
):
    rows, flat = d_re_ref.shape
    length = rows // SEGMENTS
    at = 0
    for ref in (gate_ref, up_ref, down_ref):
        weight_ref[:, at : at + ref.shape[1]] = ref[...]
        at += ref.shape[1]
    bar, ratio = rates(decay_ref, freq_ref, log_step_ref)
    fill_drive(x_ref, b_re_ref, b_im_ref, xf_ref, xp_ref, d_re_ref, d_im_ref)
    lam = tuple(jnp.broadcast_to(part, (SEGMENTS, flat)) for part in bar)

    def advance(j, state):
        at = pl.ds(pl.multiple_of(j * SEGMENTS, SEGMENTS), SEGMENTS)
        return plus(times(lam, state), (d_re_ref[at, :], d_im_ref[at, :]))

    zero = jnp.zeros((SEGMENTS, flat), F32)
    ends = lax.fori_loop(0, length, advance, (zero, zero), unroll=4)
    over = squared(bar, bits(length))
    carry = jnp.zeros((1, flat), F32), jnp.zeros((1, flat), F32)
    for s in range(SEGMENTS):
        seg_ref[0, s : s + 1, :], seg_ref[1, s : s + 1, :] = carry
        carry = plus(times(over, carry), tuple(part[s : s + 1, :] for part in ends))
    for i, part in enumerate((*bar, *ratio)):
        row_ref[i : i + 1, :] = part
    block = tuple(as_tile(part) for part in squared(over, bits(SEGMENTS)))
    state = tuple(as_tile(part) for part in carry)
    me = me_ref[0]
    for place in range(end_ref.shape[0]):
        later = place > me
        sent = jnp.concatenate(state, axis=0)
        end_ref[place] = jnp.where(later, sent, 0.0).astype(BF16)
        state = tuple(
            jnp.where(later, new, old) for new, old in zip(times(block, state), state)
        )


def local_kernel(
    row_ref, seg_ref, x_ref, b_re_ref, b_im_ref, c_re_ref, c_im_ref, skip_ref,
    y_ref, power_ref,
    xf_ref, xp_ref, d_re_ref, d_im_ref, s_ref, w_ref,
):
    rows, flat = d_re_ref.shape
    length = rows // SEGMENTS
    fill_drive(x_ref, b_re_ref, b_im_ref, xf_ref, xp_ref, d_re_ref, d_im_ref)
    bar = row_ref[0:1, :], row_ref[1:2, :]
    ratio = row_ref[2:3, :], row_ref[3:4, :]
    lam = tuple(jnp.broadcast_to(part, (SEGMENTS, flat)) for part in bar)

    def advance(j, state):
        at = pl.ds(pl.multiple_of(j * 2 * SEGMENTS, 2 * SEGMENTS), 2 * SEGMENTS)
        d_re, d_im = d_re_ref[at, :], d_im_ref[at, :]
        first = plus(times(lam, state), (d_re[:SEGMENTS], d_im[:SEGMENTS]))
        second = plus(times(lam, first), (d_re[SEGMENTS:], d_im[SEGMENTS:]))
        for i in (0, 1):
            both = jnp.concatenate([first[i], second[i]], axis=0)
            s_ref[at, i * flat : (i + 1) * flat] = both.astype(BF16)
        return second

    lax.fori_loop(0, length // 2, advance, (seg_ref[0], seg_ref[1]), unroll=2)
    over = squared(bar, bits(length))
    power = jnp.ones((1, flat), F32), jnp.zeros((1, flat), F32)
    for s in range(SEGMENTS):
        w_ref[0, s : s + 1, :], w_ref[1, s : s + 1, :] = power
        power = times(power, over)

    def raise_power(j, power):
        at = pl.ds(pl.multiple_of(j * 2 * SEGMENTS, 2 * SEGMENTS), 2 * SEGMENTS)
        first = times(lam, power)
        second = times(lam, first)
        for i in (0, 1):
            both = jnp.concatenate([first[i], second[i]], axis=0)
            power_ref[at, i * flat : (i + 1) * flat] = both.astype(BF16)
        return second

    lax.fori_loop(0, length // 2, raise_power, (w_ref[0], w_ref[1]), unroll=2)
    read = wide_read(c_re_ref, c_im_ref, ratio)
    out = lax.dot_general(s_ref[...], read, NT, preferred_element_type=F32)
    y_ref[...] = out + skip_ref[...] * xp_ref[...]


def finish_kernel(
    piece_ref, row_ref, c_re_ref, c_im_ref, y_ref, power_ref, out_ref, t_ref
):
    pieces = jnp.sum(piece_ref[...].astype(F32), axis=0)
    half = pieces.shape[0] // 2
    total = from_tile(pieces[:half]), from_tile(pieces[half:])
    ratio = row_ref[2:3, :], row_ref[3:4, :]
    read = wide_read(c_re_ref, c_im_ref, times(ratio, total))
    y = y_ref[...] + lax.dot_general(power_ref[...], read, NT, preferred_element_type=F32)
    y = jax.nn.gelu(y, approximate=True)
    length = y.shape[0] // SEGMENTS
    for i in range(y.shape[1] // LANES):
        at = slice(i * LANES, (i + 1) * LANES)
        for j in range(length):
            t_ref[i, pl.ds(j, SEGMENTS, stride=length), :] = y[
                j * SEGMENTS : (j + 1) * SEGMENTS, at
            ]
        out_ref[:, at] = t_ref[i].astype(BF16)


def shaped(*shape, dtype=F32):
    return jax.ShapeDtypeStruct(shape, dtype)


def activations(
    state_input, decay_real, frequency, log_step, drive_real, drive_imag,
    read_real, read_imag, skip_gain, weights,
):
    rows, chans = state_input.shape
    groups, states = decay_real.shape
    flat = groups * states
    peers = lax.axis_size("sp")
    me = lax.axis_index("sp").reshape(1)
    log_row = log_step.reshape(1, groups)
    b = [part.transpose(0, 2, 1).reshape(chans, states) for part in (drive_real, drive_imag)]
    c = [part.reshape(chans, states) for part in (read_real, read_imag)]
    skip = skip_gain.reshape(1, chans)
    drive_scratch = [
        pltpu.VMEM((chans // LANES, rows, LANES), F32),
        pltpu.VMEM((rows, chans), F32),
        pltpu.VMEM((rows, flat), F32),
        pltpu.VMEM((rows, flat), F32),
    ]
    whole = pl.BlockSpec(memory_space=pltpu.VMEM)
    end, seg, row, weight = pl.pallas_call(
        ends_kernel,
        out_shape=(
            shaped(peers, 2 * flat // LANES, LANES, dtype=BF16),
            shaped(2, SEGMENTS, flat),
            shaped(4, flat),
            shaped(weights[0].shape[0], sum(w.shape[1] for w in weights), dtype=BF16),
        ),
        in_specs=[pl.BlockSpec(memory_space=pltpu.SMEM), *[whole] * 9],
        scratch_shapes=drive_scratch,
        name="ssm_ends",
    )(me, decay_real, frequency, log_row, state_input, *b, *weights)
    weight = lax.all_gather(weight, "sp", axis=0, tiled=True)
    pieces = lax.all_to_all(end, "sp", 0, 0, tiled=True)
    local, power = pl.pallas_call(
        local_kernel,
        out_shape=(shaped(rows, chans), shaped(rows, 2 * flat, dtype=BF16)),
        scratch_shapes=[
            *drive_scratch,
            pltpu.VMEM((rows, 2 * flat), BF16),
            pltpu.VMEM((2, SEGMENTS, flat), F32),
        ],
        cost_estimate=pl.CostEstimate(
            flops=8 * rows * flat * chans, bytes_accessed=8 * rows * flat, transcendentals=0
        ),
        name="ssm_local",
    )(row, seg, state_input, *b, *c, skip)
    acts = pl.pallas_call(
        finish_kernel,
        out_shape=shaped(rows, chans, dtype=BF16),
        scratch_shapes=[pltpu.VMEM((chans // LANES, rows, LANES), F32)],
        name="ssm_finish",
    )(pieces, row, *c, local, power)
    return acts, weight


def ring(array, by):
    peers = lax.axis_size("tp")
    return lax.ppermute(array, "tp", [(i, (i + by) % peers) for i in range(peers)])


def rows_at(array, index, size):
    return lax.dynamic_slice_in_dim(array, index * size, size, 0)


def gathered(own):
    half = own.shape[0] // 2
    left = ring(own, 1)
    right = ring(own, -1)
    far_top = ring(left[:half], 1)
    far_low = ring(right[half:], -1)
    return own, left, right, jnp.concatenate([far_top, far_low], axis=0)


def summed(far, right, left, own):
    half = own.shape[0] // 2
    from_left_low = ring(right[half:].astype(BF16), 1)
    from_right_top = ring(left[:half].astype(BF16), -1)
    far = far.astype(BF16)
    passing_up = ring(far[:half], 1)
    passing_down = ring(far[half:], -1)
    from_left_top = ring((right[:half] + passing_up.astype(F32)).astype(BF16), 1)
    from_right_low = ring((left[half:] + passing_down.astype(F32)).astype(BF16), -1)
    top = own[:half] + from_right_top.astype(F32) + from_left_top.astype(F32)
    low = own[half:] + from_left_low.astype(F32) + from_right_low.astype(F32)
    return jnp.concatenate([top, low], axis=0)


def shards(
    residual, state_input, gate_input, decay_real, frequency, log_step,
    drive_real, drive_imag, read_real, read_imag, skip_gain,
    value_weight, glu_weight, mix_weight, norm_gain, mlp_gate, mlp_up, mlp_down,
):
    peers, me = lax.axis_size("tp"), lax.axis_index("tp")
    assert peers == 4
    hidden_width = mlp_gate.shape[1]
    chans = state_input.shape[1]
    acts, weight = activations(
        state_input, decay_real, frequency, log_step, drive_real, drive_imag,
        read_real, read_imag, skip_gain, (mlp_gate, mlp_up, mlp_down.T),
    )
    both, down_weight = weight[:, : 2 * hidden_width], weight[:, 2 * hidden_width :]
    places = dict(zip((0, 3, 1, 2), (acts, ring(acts, 1), ring(acts, -1), ring(acts, 2))))

    def project(w):
        total = None
        for place, rows in places.items():
            part = jnp.dot(
                rows, rows_at(w, (me + place) % peers, chans), preferred_element_type=F32
            )
            total = part if total is None else total + part
        return total

    value, gated = project(value_weight), project(glu_weight)
    mixed = (jax.nn.sigmoid(gate_input.astype(F32)) * value * jax.nn.sigmoid(gated)).astype(BF16)

    owned = residual.shape[0]

    def mix(place):
        rows = rows_at(mixed, (me + place) % peers, owned)
        return jnp.dot(rows, mix_weight, preferred_element_type=F32)

    far = mix(2)
    branch = summed(far, mix(1), mix(3), mix(0))
    inner = residual.astype(F32) + branch
    scale = lax.rsqrt(jnp.mean(inner * inner, axis=-1, keepdims=True) + EPSILON)
    normed = (inner * scale * norm_gain).astype(BF16)
    own, left, right, far = gathered(normed)

    def feed(rows):
        hidden = jnp.dot(rows, both, preferred_element_type=F32)
        hidden = (jax.nn.silu(hidden[:, :hidden_width]) * hidden[:, hidden_width:]).astype(BF16)
        return lax.dot_general(hidden, down_weight, NT, preferred_element_type=F32)

    near = feed(own)
    sides = feed(jnp.concatenate([left, right], axis=0))
    sides = lax.optimization_barrier(sides)
    down = summed(feed(far), sides[owned:], sides[:owned], near)
    return (inner + 0.5 * down).astype(BF16)


def solution(mesh):
    placed = (
        P(("grp", "sp", "tp"), None),
        P(("grp", "sp"), "tp"),
        P(("grp", "sp"), "tp"),
        P("tp", None),
        P("tp", None),
        P("tp"),
        P("tp", None, None),
        P("tp", None, None),
        P("tp", None, None),
        P("tp", None, None),
        P("tp"),
        P(None, "tp"),
        P(None, "tp"),
        P("tp", None),
        P(),
        P("sp", "tp"),
        P("sp", "tp"),
        P("tp", "sp"),
    )

    return jax.shard_map(
        shards, mesh=mesh, in_specs=placed, out_specs=P(("grp", "sp", "tp"), None), check_vma=False
    )
```

```python
import jax
import jax.numpy as jnp
from jax import lax
from jax.experimental import pallas as pl
from jax.experimental.pallas import tpu as pltpu
from jax.sharding import PartitionSpec as P

EPSILON = 1e-06
SEGMENTS = 8
LANES = 128
F32 = jnp.float32
BF16 = jnp.bfloat16
NT = (((1,), (1,)), ((), ()))


def times(a, b):
    return a[0] * b[0] - a[1] * b[1], a[0] * b[1] + a[1] * b[0]


def plus(a, b):
    return a[0] + b[0], a[1] + b[1]


def squared(a, count):
    for _ in range(count):
        a = times(a, a)
    return a


def iota(shape, dim):
    return lax.broadcasted_iota(jnp.int32, shape, dim)


def bits(size):
    assert size & (size - 1) == 0
    return size.bit_length() - 1


def along_lanes(x, count):
    while x.shape[1] % 128 and count > 1:
        x, count = jnp.concatenate([x, x], axis=1), count // 2
    return jnp.concatenate([x] * count, axis=1) if count > 1 else x


def as_row(x):
    groups, states = x.shape
    wide = along_lanes(x, groups)
    own = iota(wide.shape, 1) >> bits(states) == iota(wide.shape, 0)
    return jnp.sum(jnp.where(own, wide, 0.0), axis=0, keepdims=True)


def rates(decay_ref, freq_ref, log_step_ref):
    decay, freq = decay_ref[...], freq_ref[...]
    groups = decay.shape[0]
    wide = jnp.broadcast_to(log_step_ref[...], (groups, groups))
    same = iota(wide.shape, 0) == iota(wide.shape, 1)
    step = jnp.exp(jnp.sum(jnp.where(same, wide, 0.0), axis=1, keepdims=True))
    size = jnp.exp(decay * step)
    x = freq * step
    q = x * x
    cos = 1.0 + q * (-1 / 2 + q * (1 / 24 + q * (-1 / 720 + q * (1 / 40320 - q / 3628800))))
    sin = x * (1.0 + q * (-1 / 6 + q * (1 / 120 + q * (-1 / 5040 + q / 362880))))
    bar = size * cos, size * sin
    modulus = decay * decay + freq * freq
    ratio = (
        ((bar[0] - 1.0) * decay + bar[1] * freq) / modulus,
        (bar[1] * decay - (bar[0] - 1.0) * freq) / modulus,
    )
    return (as_row(bar[0]), as_row(bar[1])), (as_row(ratio[0]), as_row(ratio[1]))


def fill_drive(x_ref, b_re_ref, b_im_ref, xf_ref, xp_ref, d_re_ref, d_im_ref):
    rows, chans = x_ref.shape
    states = b_re_ref.shape[1]
    flat = d_re_ref.shape[1]
    groups = flat // states
    length = rows // SEGMENTS
    for i in range(chans // LANES):
        at = slice(i * LANES, (i + 1) * LANES)
        xf_ref[i] = x_ref[:, at].astype(F32)

        def permute(j, _, i=i, at=at):
            to = pl.ds(pl.multiple_of(j * SEGMENTS, SEGMENTS), SEGMENTS)
            xp_ref[to, at] = xf_ref[i, pl.ds(j, SEGMENTS, stride=length), :]
            return 0

        lax.fori_loop(0, length, permute, 0, unroll=8)
    x = xp_ref[...].astype(BF16)
    shape = (chans, flat)
    own = iota(shape, 0) >> bits(chans // groups) == iota(shape, 1) >> bits(states)
    for b_ref, d_ref in ((b_re_ref, d_re_ref), (b_im_ref, d_im_ref)):
        wide = jnp.where(own, along_lanes(b_ref[...], groups), 0.0).astype(BF16)
        d_ref[...] = jnp.dot(x, wide, preferred_element_type=F32)


def wide_read(c_re_ref, c_im_ref, factor):
    chans, states = c_re_ref.shape
    flat = factor[0].shape[1]
    groups = flat // states
    width = chans // groups
    shape = (chans, flat)
    own = iota(shape, 0) >> bits(width) == iota(shape, 1) >> bits(states)
    c = along_lanes(c_re_ref[...], groups), along_lanes(c_im_ref[...], groups)
    re, im = times(c, factor)
    return jnp.concatenate(
        [jnp.where(own, re, 0.0).astype(BF16), jnp.where(own, -im, 0.0).astype(BF16)], axis=1
    )


def as_tile(row):
    return jnp.concatenate(
        [row[:, i : i + LANES] for i in range(0, row.shape[1], LANES)], axis=0
    )


def from_tile(tile):
    return jnp.concatenate([tile[i : i + 1, :] for i in range(tile.shape[0])], axis=1)


def ends_kernel(
    me_ref, decay_ref, freq_ref, log_step_ref, x_ref, b_re_ref, b_im_ref,
    gate_ref, up_ref, down_ref,
    end_ref, seg_ref, row_ref, weight_ref,
    xf_ref, xp_ref, d_re_ref, d_im_ref, sems,
):
    rows, flat = d_re_ref.shape
    length = rows // SEGMENTS
    at, copies = 0, []
    for i, ref in enumerate((gate_ref, up_ref, down_ref)):
        to = weight_ref.at[:, at : at + ref.shape[1]]
        copies.append(pltpu.make_async_copy(ref, to, sems.at[i]))
        copies[-1].start()
        at += ref.shape[1]
    bar, ratio = rates(decay_ref, freq_ref, log_step_ref)
    fill_drive(x_ref, b_re_ref, b_im_ref, xf_ref, xp_ref, d_re_ref, d_im_ref)
    lam = tuple(jnp.broadcast_to(part, (SEGMENTS, flat)) for part in bar)

    def advance(j, state):
        at = pl.ds(pl.multiple_of(j * SEGMENTS, SEGMENTS), SEGMENTS)
        return plus(times(lam, state), (d_re_ref[at, :], d_im_ref[at, :]))

    zero = jnp.zeros((SEGMENTS, flat), F32)
    ends = lax.fori_loop(0, length, advance, (zero, zero), unroll=4)
    over = squared(bar, bits(length))
    carry = jnp.zeros((1, flat), F32), jnp.zeros((1, flat), F32)
    for s in range(SEGMENTS):
        seg_ref[0, s : s + 1, :], seg_ref[1, s : s + 1, :] = carry
        carry = plus(times(over, carry), tuple(part[s : s + 1, :] for part in ends))
    for i, part in enumerate((*bar, *ratio)):
        row_ref[i : i + 1, :] = part
    block = tuple(as_tile(part) for part in squared(over, bits(SEGMENTS)))
    state = tuple(as_tile(part) for part in carry)
    me = me_ref[0]
    for place in range(end_ref.shape[0]):
        later = place > me
        sent = jnp.concatenate(state, axis=0)
        end_ref[place] = jnp.where(later, sent, 0.0).astype(BF16)
        state = tuple(
            jnp.where(later, new, old) for new, old in zip(times(block, state), state)
        )
    for copy in copies:
        copy.wait()


def local_kernel(
    row_ref, seg_ref, x_ref, b_re_ref, b_im_ref, c_re_ref, c_im_ref, skip_ref,
    y_ref, power_ref,
    xf_ref, xp_ref, d_re_ref, d_im_ref, s_ref, w_ref,
):
    rows, flat = d_re_ref.shape
    length = rows // SEGMENTS
    fill_drive(x_ref, b_re_ref, b_im_ref, xf_ref, xp_ref, d_re_ref, d_im_ref)
    bar = row_ref[0:1, :], row_ref[1:2, :]
    ratio = row_ref[2:3, :], row_ref[3:4, :]
    lam = tuple(jnp.broadcast_to(part, (SEGMENTS, flat)) for part in bar)

    def advance(j, state):
        at = pl.ds(pl.multiple_of(j * 2 * SEGMENTS, 2 * SEGMENTS), 2 * SEGMENTS)
        d_re, d_im = d_re_ref[at, :], d_im_ref[at, :]
        first = plus(times(lam, state), (d_re[:SEGMENTS], d_im[:SEGMENTS]))
        second = plus(times(lam, first), (d_re[SEGMENTS:], d_im[SEGMENTS:]))
        for i in (0, 1):
            both = jnp.concatenate([first[i], second[i]], axis=0)
            s_ref[at, i * flat : (i + 1) * flat] = both.astype(BF16)
        return second

    lax.fori_loop(0, length // 2, advance, (seg_ref[0], seg_ref[1]), unroll=2)
    over = squared(bar, bits(length))
    power = jnp.ones((1, flat), F32), jnp.zeros((1, flat), F32)
    for s in range(SEGMENTS):
        w_ref[0, s : s + 1, :], w_ref[1, s : s + 1, :] = power
        power = times(power, over)

    def raise_power(j, power):
        at = pl.ds(pl.multiple_of(j * 2 * SEGMENTS, 2 * SEGMENTS), 2 * SEGMENTS)
        first = times(lam, power)
        second = times(lam, first)
        for i in (0, 1):
            both = jnp.concatenate([first[i], second[i]], axis=0)
            power_ref[at, i * flat : (i + 1) * flat] = both.astype(BF16)
        return second

    lax.fori_loop(0, length // 2, raise_power, (w_ref[0], w_ref[1]), unroll=2)
    read = wide_read(c_re_ref, c_im_ref, ratio)
    out = lax.dot_general(s_ref[...], read, NT, preferred_element_type=F32)
    y_ref[...] = out + skip_ref[...] * xp_ref[...]


def finish_kernel(
    piece_ref, row_ref, c_re_ref, c_im_ref, local_ref, powers_ref, out_ref,
    t_ref, y_ref, power_ref, sems,
):
    copies = [
        pltpu.make_async_copy(powers_ref, power_ref, sems.at[0]),
        pltpu.make_async_copy(local_ref, y_ref, sems.at[1]),
    ]
    for copy in copies:
        copy.start()
    pieces = jnp.sum(piece_ref[...].astype(F32), axis=0)
    half = pieces.shape[0] // 2
    total = from_tile(pieces[:half]), from_tile(pieces[half:])
    ratio = row_ref[2:3, :], row_ref[3:4, :]
    read = wide_read(c_re_ref, c_im_ref, times(ratio, total))
    for copy in copies:
        copy.wait()
    y = y_ref[...] + lax.dot_general(power_ref[...], read, NT, preferred_element_type=F32)
    y = jax.nn.gelu(y, approximate=True)
    length = y.shape[0] // SEGMENTS
    for i in range(y.shape[1] // LANES):
        at = slice(i * LANES, (i + 1) * LANES)
        for j in range(length):
            t_ref[i, pl.ds(j, SEGMENTS, stride=length), :] = y[
                j * SEGMENTS : (j + 1) * SEGMENTS, at
            ]
        out_ref[:, at] = t_ref[i].astype(BF16)


def shaped(*shape, dtype=F32):
    return jax.ShapeDtypeStruct(shape, dtype)


def activations(
    state_input, decay_real, frequency, log_step, drive_real, drive_imag,
    read_real, read_imag, skip_gain, weights,
):
    rows, chans = state_input.shape
    groups, states = decay_real.shape
    flat = groups * states
    peers = lax.axis_size("sp")
    me = lax.axis_index("sp").reshape(1)
    log_row = log_step.reshape(1, groups)
    b = [part.transpose(0, 2, 1).reshape(chans, states) for part in (drive_real, drive_imag)]
    c = [part.reshape(chans, states) for part in (read_real, read_imag)]
    skip = skip_gain.reshape(1, chans)
    drive_scratch = [
        pltpu.VMEM((chans // LANES, rows, LANES), F32),
        pltpu.VMEM((rows, chans), F32),
        pltpu.VMEM((rows, flat), F32),
        pltpu.VMEM((rows, flat), F32),
    ]
    whole = pl.BlockSpec(memory_space=pltpu.VMEM)
    stored = pl.BlockSpec(memory_space=pl.ANY)
    end, seg, row, weight = pl.pallas_call(
        ends_kernel,
        out_shape=(
            shaped(peers, 2 * flat // LANES, LANES, dtype=BF16),
            shaped(2, SEGMENTS, flat),
            shaped(4, flat),
            shaped(weights[0].shape[0], sum(w.shape[1] for w in weights), dtype=BF16),
        ),
        in_specs=[pl.BlockSpec(memory_space=pltpu.SMEM), *[whole] * 6, *[stored] * 3],
        out_specs=(whole, whole, whole, stored),
        scratch_shapes=[*drive_scratch, pltpu.SemaphoreType.DMA((3,))],
        name="ssm_ends",
    )(me, decay_real, frequency, log_row, state_input, *b, *weights)
    weight = lax.all_gather(weight, "sp", axis=0, tiled=True)
    pieces = lax.all_to_all(end, "sp", 0, 0, tiled=True)
    local, power = pl.pallas_call(
        local_kernel,
        out_shape=(shaped(rows, chans), shaped(rows, 2 * flat, dtype=BF16)),
        scratch_shapes=[
            *drive_scratch,
            pltpu.VMEM((rows, 2 * flat), BF16),
            pltpu.VMEM((2, SEGMENTS, flat), F32),
        ],
        cost_estimate=pl.CostEstimate(
            flops=8 * rows * flat * chans, bytes_accessed=8 * rows * flat, transcendentals=0
        ),
        name="ssm_local",
    )(row, seg, state_input, *b, *c, skip)
    acts = pl.pallas_call(
        finish_kernel,
        out_shape=shaped(rows, chans, dtype=BF16),
        in_specs=[*[whole] * 4, stored, stored],
        out_specs=whole,
        scratch_shapes=[
            pltpu.VMEM((chans // LANES, rows, LANES), F32),
            pltpu.VMEM((rows, chans), F32),
            pltpu.VMEM((rows, 2 * flat), BF16),
            pltpu.SemaphoreType.DMA((2,)),
        ],
        name="ssm_finish",
    )(pieces, row, *c, local, power)
    return acts, weight


def ring(array, by):
    peers = lax.axis_size("tp")
    return lax.ppermute(array, "tp", [(i, (i + by) % peers) for i in range(peers)])


def rows_at(array, index, size):
    return lax.dynamic_slice_in_dim(array, index * size, size, 0)


def gathered(own):
    left, right = ring(own, 1), ring(own, -1)
    far = ring(own, 2)
    return own, left, right, far


def summed(far, right, left, own):
    half = own.shape[0] // 2
    from_left_low = ring(right[half:].astype(BF16), 1)
    from_right_top = ring(left[:half].astype(BF16), -1)
    far = far.astype(BF16)
    passing_up = ring(far[:half], 1)
    passing_down = ring(far[half:], -1)
    from_left_top = ring((right[:half] + passing_up.astype(F32)).astype(BF16), 1)
    from_right_low = ring((left[half:] + passing_down.astype(F32)).astype(BF16), -1)
    top = own[:half] + from_right_top.astype(F32) + from_left_top.astype(F32)
    low = own[half:] + from_left_low.astype(F32) + from_right_low.astype(F32)
    return jnp.concatenate([top, low], axis=0)


def shards(
    residual, state_input, gate_input, decay_real, frequency, log_step,
    drive_real, drive_imag, read_real, read_imag, skip_gain,
    value_weight, glu_weight, mix_weight, norm_gain, mlp_gate, mlp_up, mlp_down,
):
    peers, me = lax.axis_size("tp"), lax.axis_index("tp")
    assert peers == 4
    hidden_width = mlp_gate.shape[1]
    chans = state_input.shape[1]
    acts, weight = activations(
        state_input, decay_real, frequency, log_step, drive_real, drive_imag,
        read_real, read_imag, skip_gain, (mlp_gate, mlp_up, mlp_down.T),
    )
    both, down_weight = weight[:, : 2 * hidden_width], weight[:, 2 * hidden_width :]
    places = dict(zip((0, 3, 1, 2), gathered(acts)))

    def project(w):
        total = None
        for place, rows in places.items():
            part = jnp.dot(
                rows, rows_at(w, (me + place) % peers, chans), preferred_element_type=F32
            )
            total = part if total is None else total + part
        return total

    value, gated = project(value_weight), project(glu_weight)
    mixed = (jax.nn.sigmoid(gate_input.astype(F32)) * value * jax.nn.sigmoid(gated)).astype(BF16)

    owned = residual.shape[0]

    def mix(place):
        rows = rows_at(mixed, (me + place) % peers, owned)
        return jnp.dot(rows, mix_weight, preferred_element_type=F32)

    far = mix(2)
    branch = summed(far, mix(1), mix(3), mix(0))
    inner = residual.astype(F32) + branch
    scale = lax.rsqrt(jnp.mean(inner * inner, axis=-1, keepdims=True) + EPSILON)
    normed = (inner * scale * norm_gain).astype(BF16)
    own, left, right, far = gathered(normed)

    def feed(rows):
        hidden = jnp.dot(rows, both, preferred_element_type=F32)
        hidden = (jax.nn.silu(hidden[:, :hidden_width]) * hidden[:, hidden_width:]).astype(BF16)
        return lax.dot_general(hidden, down_weight, NT, preferred_element_type=F32)

    sides = feed(jnp.concatenate([left, right], axis=0))
    sides = lax.optimization_barrier(sides)
    down = summed(feed(far), sides[owned:], sides[:owned], feed(own))
    return (inner + 0.5 * down).astype(BF16)


def solution(mesh):
    placed = (
        P(("grp", "sp", "tp"), None),
        P(("grp", "sp"), "tp"),
        P(("grp", "sp"), "tp"),
        P("tp", None),
        P("tp", None),
        P("tp"),
        P("tp", None, None),
        P("tp", None, None),
        P("tp", None, None),
        P("tp", None, None),
        P("tp"),
        P(None, "tp"),
        P(None, "tp"),
        P("tp", None),
        P(),
        P("sp", "tp"),
        P("sp", "tp"),
        P("tp", "sp"),
    )

    return jax.shard_map(
        shards, mesh=mesh, in_specs=placed, out_specs=P(("grp", "sp", "tp"), None), check_vma=False
    )
```

```python
import jax
import jax.numpy as jnp
from jax import lax
from jax.experimental import pallas as pl
from jax.experimental.pallas import tpu as pltpu
from jax.sharding import PartitionSpec as P

EPSILON = 1e-06
SEGMENTS = 8
LANES = 128
PART = 32
F32 = jnp.float32
BF16 = jnp.bfloat16
NT = (((1,), (1,)), ((), ()))


def times(a, b):
    return a[0] * b[0] - a[1] * b[1], a[0] * b[1] + a[1] * b[0]


def plus(a, b):
    return a[0] + b[0], a[1] + b[1]


def squared(a, count):
    for _ in range(count):
        a = times(a, a)
    return a


def iota(shape, dim):
    return lax.broadcasted_iota(jnp.int32, shape, dim)


def bits(size):
    assert size & (size - 1) == 0
    return size.bit_length() - 1


def along_lanes(x, count):
    while x.shape[1] % 128 and count > 1:
        x, count = jnp.concatenate([x, x], axis=1), count // 2
    return jnp.concatenate([x] * count, axis=1) if count > 1 else x


def as_row(x):
    groups, states = x.shape
    wide = along_lanes(x, groups)
    own = iota(wide.shape, 1) >> bits(states) == iota(wide.shape, 0)
    return jnp.sum(jnp.where(own, wide, 0.0), axis=0, keepdims=True)


def rates(decay_ref, freq_ref, log_step_ref):
    decay, freq = decay_ref[...], freq_ref[...]
    groups = decay.shape[0]
    wide = jnp.broadcast_to(log_step_ref[...], (groups, groups))
    same = iota(wide.shape, 0) == iota(wide.shape, 1)
    step = jnp.exp(jnp.sum(jnp.where(same, wide, 0.0), axis=1, keepdims=True))
    size = jnp.exp(decay * step)
    x = freq * step
    q = x * x
    cos = 1.0 + q * (-1 / 2 + q * (1 / 24 + q * (-1 / 720 + q * (1 / 40320 - q / 3628800))))
    sin = x * (1.0 + q * (-1 / 6 + q * (1 / 120 + q * (-1 / 5040 + q / 362880))))
    bar = size * cos, size * sin
    modulus = decay * decay + freq * freq
    ratio = (
        ((bar[0] - 1.0) * decay + bar[1] * freq) / modulus,
        (bar[1] * decay - (bar[0] - 1.0) * freq) / modulus,
    )
    return (as_row(bar[0]), as_row(bar[1])), (as_row(ratio[0]), as_row(ratio[1]))


def fill_drive(x_ref, b_re_ref, b_im_ref, xf_ref, xp_ref, d_re_ref, d_im_ref, wide_ref):
    rows, chans = x_ref.shape
    states = b_re_ref.shape[1]
    flat = d_re_ref.shape[1]
    groups = flat // states
    length = rows // SEGMENTS
    for i in range(chans // LANES):
        at = slice(i * LANES, (i + 1) * LANES)
        xf_ref[i] = x_ref[:, at].astype(F32)

        def permute(j, _, i=i, at=at):
            to = pl.ds(pl.multiple_of(j * SEGMENTS, SEGMENTS), SEGMENTS)
            xp_ref[to, at] = xf_ref[i, pl.ds(j, SEGMENTS, stride=length), :]
            return 0

        lax.fori_loop(0, length, permute, 0, unroll=8)
    x = xp_ref[...].astype(BF16)
    for b_ref, d_ref in ((b_re_ref, d_re_ref), (b_im_ref, d_im_ref)):

        def widen(i, _, b_ref=b_ref):
            at = pl.ds(pl.multiple_of(i * PART, PART), PART)
            wide = along_lanes(b_ref[at, :], groups)
            own = (iota(wide.shape, 0) + i * PART) >> bits(chans // groups)
            own = own == iota(wide.shape, 1) >> bits(states)
            wide_ref[at, :] = jnp.where(own, wide, 0.0).astype(BF16)
            return 0

        lax.fori_loop(0, chans // PART, widen, 0)
        d_ref[...] = jnp.dot(x, wide_ref[...], preferred_element_type=F32)


def wide_read(c_re_ref, c_im_ref, factor, read_ref):
    chans, states = c_re_ref.shape
    flat = factor[0].shape[1]
    groups = flat // states
    width = chans // groups

    def widen(i, _):
        at = pl.ds(pl.multiple_of(i * PART, PART), PART)
        c = along_lanes(c_re_ref[at, :], groups), along_lanes(c_im_ref[at, :], groups)
        re, im = times(c, factor)
        own = (iota(re.shape, 0) + i * PART) >> bits(width) == iota(re.shape, 1) >> bits(states)
        read_ref[at, :flat] = jnp.where(own, re, 0.0).astype(BF16)
        read_ref[at, flat:] = jnp.where(own, -im, 0.0).astype(BF16)
        return 0

    lax.fori_loop(0, chans // PART, widen, 0)


def as_tile(row):
    return jnp.concatenate(
        [row[:, i : i + LANES] for i in range(0, row.shape[1], LANES)], axis=0
    )


def from_tile(tile):
    return jnp.concatenate([tile[i : i + 1, :] for i in range(tile.shape[0])], axis=1)


def ends_kernel(
    me_ref, decay_ref, freq_ref, log_step_ref, x_ref, b_re_ref, b_im_ref,
    gate_ref, up_ref, down_ref,
    end_ref, seg_ref, row_ref, weight_ref,
    xf_ref, xp_ref, d_re_ref, d_im_ref, wide_ref,
):
    rows, flat = d_re_ref.shape
    length = rows // SEGMENTS
    at = 0
    for ref in (gate_ref, up_ref, down_ref):
        weight_ref[:, at : at + ref.shape[1]] = ref[...]
        at += ref.shape[1]
    bar, ratio = rates(decay_ref, freq_ref, log_step_ref)
    fill_drive(x_ref, b_re_ref, b_im_ref, xf_ref, xp_ref, d_re_ref, d_im_ref, wide_ref)
    lam = tuple(jnp.broadcast_to(part, (SEGMENTS, flat)) for part in bar)

    def advance(j, state):
        at = pl.ds(pl.multiple_of(j * SEGMENTS, SEGMENTS), SEGMENTS)
        return plus(times(lam, state), (d_re_ref[at, :], d_im_ref[at, :]))

    zero = jnp.zeros((SEGMENTS, flat), F32)
    ends = lax.fori_loop(0, length, advance, (zero, zero), unroll=2)
    over = squared(bar, bits(length))
    carry = jnp.zeros((1, flat), F32), jnp.zeros((1, flat), F32)
    for s in range(SEGMENTS):
        seg_ref[0, s : s + 1, :], seg_ref[1, s : s + 1, :] = carry
        carry = plus(times(over, carry), tuple(part[s : s + 1, :] for part in ends))
    for i, part in enumerate((*bar, *ratio)):
        row_ref[i : i + 1, :] = part
    block = tuple(as_tile(part) for part in squared(over, bits(SEGMENTS)))
    state = tuple(as_tile(part) for part in carry)
    me = me_ref[0]
    for place in range(end_ref.shape[0]):
        later = place > me
        sent = jnp.concatenate(state, axis=0)
        end_ref[place] = jnp.where(later, sent, 0.0).astype(BF16)
        state = tuple(
            jnp.where(later, new, old) for new, old in zip(times(block, state), state)
        )


def local_kernel(
    row_ref, seg_ref, x_ref, b_re_ref, b_im_ref, c_re_ref, c_im_ref, skip_ref,
    y_ref, power_ref,
    xf_ref, xp_ref, d_re_ref, d_im_ref, wide_ref, read_ref, s_ref, w_ref,
):
    rows, flat = d_re_ref.shape
    length = rows // SEGMENTS
    fill_drive(x_ref, b_re_ref, b_im_ref, xf_ref, xp_ref, d_re_ref, d_im_ref, wide_ref)
    bar = row_ref[0:1, :], row_ref[1:2, :]
    ratio = row_ref[2:3, :], row_ref[3:4, :]
    lam = tuple(jnp.broadcast_to(part, (SEGMENTS, flat)) for part in bar)

    def advance(j, state):
        at = pl.ds(pl.multiple_of(j * 2 * SEGMENTS, 2 * SEGMENTS), 2 * SEGMENTS)
        d_re, d_im = d_re_ref[at, :], d_im_ref[at, :]
        first = plus(times(lam, state), (d_re[:SEGMENTS], d_im[:SEGMENTS]))
        second = plus(times(lam, first), (d_re[SEGMENTS:], d_im[SEGMENTS:]))
        for i in (0, 1):
            both = jnp.concatenate([first[i], second[i]], axis=0)
            s_ref[at, i * flat : (i + 1) * flat] = both.astype(BF16)
        return second

    lax.fori_loop(0, length // 2, advance, (seg_ref[0], seg_ref[1]))
    over = squared(bar, bits(length))
    power = jnp.ones((1, flat), F32), jnp.zeros((1, flat), F32)
    for s in range(SEGMENTS):
        w_ref[0, s : s + 1, :], w_ref[1, s : s + 1, :] = power
        power = times(power, over)

    def raise_power(j, power):
        at = pl.ds(pl.multiple_of(j * 2 * SEGMENTS, 2 * SEGMENTS), 2 * SEGMENTS)
        first = times(lam, power)
        second = times(lam, first)
        for i in (0, 1):
            both = jnp.concatenate([first[i], second[i]], axis=0)
            power_ref[at, i * flat : (i + 1) * flat] = both.astype(BF16)
        return second

    lax.fori_loop(0, length // 2, raise_power, (w_ref[0], w_ref[1]))
    wide_read(c_re_ref, c_im_ref, ratio, read_ref)
    out = lax.dot_general(s_ref[...], read_ref[...], NT, preferred_element_type=F32)
    y_ref[...] = out + skip_ref[...] * xp_ref[...]


def finish_kernel(
    piece_ref, row_ref, c_re_ref, c_im_ref, y_ref, power_ref, out_ref, t_ref, read_ref
):
    pieces = jnp.sum(piece_ref[...].astype(F32), axis=0)
    half = pieces.shape[0] // 2
    total = from_tile(pieces[:half]), from_tile(pieces[half:])
    ratio = row_ref[2:3, :], row_ref[3:4, :]
    wide_read(c_re_ref, c_im_ref, times(ratio, total), read_ref)
    y = y_ref[...] + lax.dot_general(power_ref[...], read_ref[...], NT, preferred_element_type=F32)
    length = y.shape[0] // SEGMENTS
    y = jax.nn.gelu(y, approximate=True)
    for i in range(y.shape[1] // LANES):
        at = slice(i * LANES, (i + 1) * LANES)
        for j in range(length):
            t_ref[i, pl.ds(j, SEGMENTS, stride=length), :] = y[
                j * SEGMENTS : (j + 1) * SEGMENTS, at
            ]
        out_ref[:, at] = t_ref[i].astype(BF16)


def shaped(*shape, dtype=F32):
    return jax.ShapeDtypeStruct(shape, dtype)


def activations(
    state_input, decay_real, frequency, log_step, drive_real, drive_imag,
    read_real, read_imag, skip_gain, weights,
):
    rows, chans = state_input.shape
    groups, states = decay_real.shape
    flat = groups * states
    peers = lax.axis_size("sp")
    me = lax.axis_index("sp").reshape(1)
    log_row = log_step.reshape(1, groups)
    b = [part.transpose(0, 2, 1).reshape(chans, states) for part in (drive_real, drive_imag)]
    c = [part.reshape(chans, states) for part in (read_real, read_imag)]
    skip = skip_gain.reshape(1, chans)
    drive_scratch = [
        pltpu.VMEM((chans // LANES, rows, LANES), F32),
        pltpu.VMEM((rows, chans), F32),
        pltpu.VMEM((rows, flat), F32),
        pltpu.VMEM((rows, flat), F32),
        pltpu.VMEM((chans, flat), BF16),
    ]
    whole = pl.BlockSpec(memory_space=pltpu.VMEM)
    end, seg, row, weight = pl.pallas_call(
        ends_kernel,
        out_shape=(
            shaped(peers, 2 * flat // LANES, LANES, dtype=BF16),
            shaped(2, SEGMENTS, flat),
            shaped(4, flat),
            shaped(weights[0].shape[0], sum(w.shape[1] for w in weights), dtype=BF16),
        ),
        in_specs=[pl.BlockSpec(memory_space=pltpu.SMEM), *[whole] * 9],
        scratch_shapes=drive_scratch,
        name="ssm_ends",
    )(me, decay_real, frequency, log_row, state_input, *b, *weights)
    weight = lax.all_gather(weight, "sp", axis=0, tiled=True)
    pieces = lax.all_to_all(end, "sp", 0, 0, tiled=True)
    local, power = pl.pallas_call(
        local_kernel,
        out_shape=(shaped(rows, chans), shaped(rows, 2 * flat, dtype=BF16)),
        scratch_shapes=[
            *drive_scratch,
            pltpu.VMEM((chans, 2 * flat), BF16),
            pltpu.VMEM((rows, 2 * flat), BF16),
            pltpu.VMEM((2, SEGMENTS, flat), F32),
        ],
        cost_estimate=pl.CostEstimate(
            flops=8 * rows * flat * chans, bytes_accessed=8 * rows * flat, transcendentals=0
        ),
        name="ssm_local",
    )(row, seg, state_input, *b, *c, skip)
    acts = pl.pallas_call(
        finish_kernel,
        out_shape=shaped(rows, chans, dtype=BF16),
        scratch_shapes=[
            pltpu.VMEM((chans // LANES, rows, LANES), F32),
            pltpu.VMEM((chans, 2 * flat), BF16),
        ],
        name="ssm_finish",
    )(pieces, row, *c, local, power)
    return acts, weight


def ring(array, by):
    peers = lax.axis_size("tp")
    return lax.ppermute(array, "tp", [(i, (i + by) % peers) for i in range(peers)])


def rows_at(array, index, size):
    return lax.dynamic_slice_in_dim(array, index * size, size, 0)


def gathered(top, low):
    left_top = ring(top, 1)
    right_low = ring(low, -1)
    left_low = ring(low, 1)
    right_top = ring(top, -1)
    far_top = ring(left_top, 1)
    far_low = ring(right_low, -1)
    return (left_top, left_low), (right_top, right_low), (far_top, far_low)


def summed(far, right, left, own):
    half = own.shape[0] // 2
    from_left_low = ring(right[half:].astype(BF16), 1)
    from_right_top = ring(left[:half].astype(BF16), -1)
    far = far.astype(BF16)
    passing_up = ring(far[:half], 1)
    passing_down = ring(far[half:], -1)
    from_left_top = ring((right[:half] + passing_up.astype(F32)).astype(BF16), 1)
    from_right_low = ring((left[half:] + passing_down.astype(F32)).astype(BF16), -1)
    top = own[:half] + from_right_top.astype(F32) + from_left_top.astype(F32)
    low = own[half:] + from_left_low.astype(F32) + from_right_low.astype(F32)
    return top, low


def summed_late(far, right, left, own):
    half = own.shape[0] // 2
    far = far.astype(BF16)
    passing_up = ring(far[:half], 1)
    passing_down = ring(far[half:], -1)
    right = right + jnp.pad(passing_up, ((0, half), (0, 0))).astype(F32)
    left = left + jnp.pad(passing_down, ((half, 0), (0, 0))).astype(F32)
    from_left, from_right = ring(right.astype(BF16), 1), ring(left.astype(BF16), -1)
    total = own + from_left.astype(F32) + from_right.astype(F32)
    return total[:half], total[half:]


def shards(
    residual, state_input, gate_input, decay_real, frequency, log_step,
    drive_real, drive_imag, read_real, read_imag, skip_gain,
    value_weight, glu_weight, mix_weight, norm_gain, mlp_gate, mlp_up, mlp_down,
):
    peers, me = lax.axis_size("tp"), lax.axis_index("tp")
    assert peers == 4
    hidden_width = mlp_gate.shape[1]
    chans = state_input.shape[1]
    acts, weight = activations(
        state_input, decay_real, frequency, log_step, drive_real, drive_imag,
        read_real, read_imag, skip_gain, (mlp_gate, mlp_up, mlp_down.T),
    )
    both, down_weight = weight[:, : 2 * hidden_width], weight[:, 2 * hidden_width :]
    places = dict(
        zip((0, 3, 1, 2), (acts, ring(acts, 1), ring(acts, -1), ring(acts, 2)))
    )

    def project(w):
        total = None
        for place, rows in places.items():
            part = jnp.dot(
                rows, rows_at(w, (me + place) % peers, chans), preferred_element_type=F32
            )
            total = part if total is None else total + part
        return total

    value, gated = project(value_weight), project(glu_weight)
    mixed = (jax.nn.sigmoid(gate_input.astype(F32)) * value * jax.nn.sigmoid(gated)).astype(BF16)

    owned = residual.shape[0]

    def mix(place):
        rows = rows_at(mixed, (me + place) % peers, owned)
        return jnp.dot(rows, mix_weight, preferred_element_type=F32)

    far = mix(2)
    branch = summed(far, mix(1), mix(3), mix(0))
    half = owned // 2
    inner, normed = [], []
    for i, part in enumerate(branch):
        inner.append(residual[i * half : (i + 1) * half].astype(F32) + part)
        scale = lax.rsqrt(jnp.mean(inner[i] * inner[i], axis=-1, keepdims=True) + EPSILON)
        normed.append((inner[i] * scale * norm_gain).astype(BF16))
    left, right, far = gathered(*normed)

    def feed(rows):
        hidden = jnp.dot(rows, both, preferred_element_type=F32)
        hidden = (jax.nn.silu(hidden[:, :hidden_width]) * hidden[:, hidden_width:]).astype(BF16)
        return lax.dot_general(hidden, down_weight, NT, preferred_element_type=F32)

    sides = feed(jnp.concatenate([*left, *right], axis=0))
    far = feed(jnp.concatenate(far, axis=0))
    own = feed(jnp.concatenate(normed, axis=0))
    down = summed_late(far, sides[owned:], sides[:owned], own)
    return jnp.concatenate(
        [(i + 0.5 * part).astype(BF16) for i, part in zip(inner, down)], axis=0
    )


def solution(mesh):
    placed = (
        P(("grp", "sp", "tp"), None),
        P(("grp", "sp"), "tp"),
        P(("grp", "sp"), "tp"),
        P("tp", None),
        P("tp", None),
        P("tp"),
        P("tp", None, None),
        P("tp", None, None),
        P("tp", None, None),
        P("tp", None, None),
        P("tp"),
        P(None, "tp"),
        P(None, "tp"),
        P("tp", None),
        P(),
        P("sp", "tp"),
        P("sp", "tp"),
        P("tp", "sp"),
    )

    return jax.shard_map(
        shards, mesh=mesh, in_specs=placed, out_specs=P(("grp", "sp", "tp"), None), check_vma=False
    )
```

```python
import jax
import jax.numpy as jnp
from jax import lax
from jax.experimental import pallas as pl
from jax.experimental.pallas import tpu as pltpu
from jax.sharding import PartitionSpec as P

EPSILON = 1e-06
SEGMENTS = 8
LANES = 128
F32 = jnp.float32
BF16 = jnp.bfloat16
NT = (((1,), (1,)), ((), ()))


def times(a, b):
    return a[0] * b[0] - a[1] * b[1], a[0] * b[1] + a[1] * b[0]


def plus(a, b):
    return a[0] + b[0], a[1] + b[1]


def squared(a, count):
    for _ in range(count):
        a = times(a, a)
    return a


def iota(shape, dim):
    return lax.broadcasted_iota(jnp.int32, shape, dim)


def bits(size):
    assert size & (size - 1) == 0
    return size.bit_length() - 1


def along_lanes(x, count):
    while x.shape[1] % 128 and count > 1:
        x, count = jnp.concatenate([x, x], axis=1), count // 2
    return jnp.concatenate([x] * count, axis=1) if count > 1 else x


def as_row(x):
    groups, states = x.shape
    wide = along_lanes(x, groups)
    own = iota(wide.shape, 1) >> bits(states) == iota(wide.shape, 0)
    return jnp.sum(jnp.where(own, wide, 0.0), axis=0, keepdims=True)


def rates(decay_ref, freq_ref, log_step_ref):
    decay, freq = decay_ref[...], freq_ref[...]
    groups = decay.shape[0]
    wide = jnp.broadcast_to(log_step_ref[...], (groups, groups))
    same = iota(wide.shape, 0) == iota(wide.shape, 1)
    step = jnp.exp(jnp.sum(jnp.where(same, wide, 0.0), axis=1, keepdims=True))
    size = jnp.exp(decay * step)
    x = freq * step
    q = x * x
    cos = 1.0 + q * (-1 / 2 + q * (1 / 24 + q * (-1 / 720 + q * (1 / 40320 - q / 3628800))))
    sin = x * (1.0 + q * (-1 / 6 + q * (1 / 120 + q * (-1 / 5040 + q / 362880))))
    bar = size * cos, size * sin
    modulus = decay * decay + freq * freq
    ratio = (
        ((bar[0] - 1.0) * decay + bar[1] * freq) / modulus,
        (bar[1] * decay - (bar[0] - 1.0) * freq) / modulus,
    )
    return (as_row(bar[0]), as_row(bar[1])), (as_row(ratio[0]), as_row(ratio[1]))


def fill_drive(x_ref, b_re_ref, b_im_ref, xf_ref, xp_ref, d_re_ref, d_im_ref):
    rows, chans = x_ref.shape
    states = b_re_ref.shape[1]
    flat = d_re_ref.shape[1]
    groups = flat // states
    length = rows // SEGMENTS
    for i in range(chans // LANES):
        at = slice(i * LANES, (i + 1) * LANES)
        xf_ref[i] = x_ref[:, at].astype(F32)

        def permute(j, _, i=i, at=at):
            to = pl.ds(pl.multiple_of(j * SEGMENTS, SEGMENTS), SEGMENTS)
            xp_ref[to, at] = xf_ref[i, pl.ds(j, SEGMENTS, stride=length), :]
            return 0

        lax.fori_loop(0, length, permute, 0, unroll=8)
    x = xp_ref[...].astype(BF16)
    shape = (chans, flat)
    own = iota(shape, 0) >> bits(chans // groups) == iota(shape, 1) >> bits(states)
    for b_ref, d_ref in ((b_re_ref, d_re_ref), (b_im_ref, d_im_ref)):
        wide = jnp.where(own, along_lanes(b_ref[...], groups), 0.0).astype(BF16)
        d_ref[...] = jnp.dot(x, wide, preferred_element_type=F32)


def wide_read(c_re_ref, c_im_ref, factor):
    chans, states = c_re_ref.shape
    flat = factor[0].shape[1]
    groups = flat // states
    width = chans // groups
    shape = (chans, flat)
    own = iota(shape, 0) >> bits(width) == iota(shape, 1) >> bits(states)
    c = along_lanes(c_re_ref[...], groups), along_lanes(c_im_ref[...], groups)
    re, im = times(c, factor)
    return jnp.concatenate(
        [jnp.where(own, re, 0.0).astype(BF16), jnp.where(own, -im, 0.0).astype(BF16)], axis=1
    )


def as_tile(row):
    return jnp.concatenate(
        [row[:, i : i + LANES] for i in range(0, row.shape[1], LANES)], axis=0
    )


def from_tile(tile):
    return jnp.concatenate([tile[i : i + 1, :] for i in range(tile.shape[0])], axis=1)


def ends_kernel(
    me_ref, decay_ref, freq_ref, log_step_ref, x_ref, b_re_ref, b_im_ref,
    gate_ref, up_ref, down_ref,
    end_ref, seg_ref, row_ref, weight_ref,
    xf_ref, xp_ref, d_re_ref, d_im_ref,
):
    rows, flat = d_re_ref.shape
    length = rows // SEGMENTS
    at = 0
    for ref in (gate_ref, up_ref, down_ref):
        weight_ref[:, at : at + ref.shape[1]] = ref[...]
        at += ref.shape[1]
    bar, ratio = rates(decay_ref, freq_ref, log_step_ref)
    fill_drive(x_ref, b_re_ref, b_im_ref, xf_ref, xp_ref, d_re_ref, d_im_ref)
    lam = tuple(jnp.broadcast_to(part, (SEGMENTS, flat)) for part in bar)

    def advance(j, state):
        at = pl.ds(pl.multiple_of(j * SEGMENTS, SEGMENTS), SEGMENTS)
        return plus(times(lam, state), (d_re_ref[at, :], d_im_ref[at, :]))

    zero = jnp.zeros((SEGMENTS, flat), F32)
    ends = lax.fori_loop(0, length, advance, (zero, zero), unroll=4)
    over = squared(bar, bits(length))
    carry = jnp.zeros((1, flat), F32), jnp.zeros((1, flat), F32)
    for s in range(SEGMENTS):
        seg_ref[0, s : s + 1, :], seg_ref[1, s : s + 1, :] = carry
        carry = plus(times(over, carry), tuple(part[s : s + 1, :] for part in ends))
    for i, part in enumerate((*bar, *ratio)):
        row_ref[i : i + 1, :] = part
    block = tuple(as_tile(part) for part in squared(over, bits(SEGMENTS)))
    state = tuple(as_tile(part) for part in carry)
    me = me_ref[0]
    for place in range(end_ref.shape[0]):
        later = place > me
        sent = jnp.concatenate(state, axis=0)
        end_ref[place] = jnp.where(later, sent, 0.0).astype(BF16)
        state = tuple(
            jnp.where(later, new, old) for new, old in zip(times(block, state), state)
        )


def local_kernel(
    row_ref, seg_ref, x_ref, b_re_ref, b_im_ref, c_re_ref, c_im_ref, skip_ref,
    y_ref, power_ref,
    xf_ref, xp_ref, d_re_ref, d_im_ref, s_ref, w_ref,
):
    rows, flat = d_re_ref.shape
    length = rows // SEGMENTS
    fill_drive(x_ref, b_re_ref, b_im_ref, xf_ref, xp_ref, d_re_ref, d_im_ref)
    bar = row_ref[0:1, :], row_ref[1:2, :]
    ratio = row_ref[2:3, :], row_ref[3:4, :]
    lam = tuple(jnp.broadcast_to(part, (SEGMENTS, flat)) for part in bar)

    def advance(j, state):
        at = pl.ds(pl.multiple_of(j * 2 * SEGMENTS, 2 * SEGMENTS), 2 * SEGMENTS)
        d_re, d_im = d_re_ref[at, :], d_im_ref[at, :]
        first = plus(times(lam, state), (d_re[:SEGMENTS], d_im[:SEGMENTS]))
        second = plus(times(lam, first), (d_re[SEGMENTS:], d_im[SEGMENTS:]))
        for i in (0, 1):
            both = jnp.concatenate([first[i], second[i]], axis=0)
            s_ref[at, i * flat : (i + 1) * flat] = both.astype(BF16)
        return second

    lax.fori_loop(0, length // 2, advance, (seg_ref[0], seg_ref[1]), unroll=2)
    over = squared(bar, bits(length))
    power = jnp.ones((1, flat), F32), jnp.zeros((1, flat), F32)
    for s in range(SEGMENTS):
        w_ref[0, s : s + 1, :], w_ref[1, s : s + 1, :] = power
        power = times(power, over)

    def raise_power(j, power):
        at = pl.ds(pl.multiple_of(j * 2 * SEGMENTS, 2 * SEGMENTS), 2 * SEGMENTS)
        first = times(lam, power)
        second = times(lam, first)
        for i in (0, 1):
            both = jnp.concatenate([first[i], second[i]], axis=0)
            power_ref[at, i * flat : (i + 1) * flat] = both.astype(BF16)
        return second

    lax.fori_loop(0, length // 2, raise_power, (w_ref[0], w_ref[1]), unroll=2)
    read = wide_read(c_re_ref, c_im_ref, ratio)
    out = lax.dot_general(s_ref[...], read, NT, preferred_element_type=F32)
    y_ref[...] = out + skip_ref[...] * xp_ref[...]


def finish_kernel(
    piece_ref, row_ref, c_re_ref, c_im_ref, y_ref, power_ref, out_ref, t_ref
):
    pieces = jnp.sum(piece_ref[...].astype(F32), axis=0)
    half = pieces.shape[0] // 2
    total = from_tile(pieces[:half]), from_tile(pieces[half:])
    ratio = row_ref[2:3, :], row_ref[3:4, :]
    read = wide_read(c_re_ref, c_im_ref, times(ratio, total))
    y = y_ref[...] + lax.dot_general(power_ref[...], read, NT, preferred_element_type=F32)
    y = jax.nn.gelu(y, approximate=True)
    length = y.shape[0] // SEGMENTS
    for i in range(y.shape[1] // LANES):
        at = slice(i * LANES, (i + 1) * LANES)
        for j in range(length):
            t_ref[i, pl.ds(j, SEGMENTS, stride=length), :] = y[
                j * SEGMENTS : (j + 1) * SEGMENTS, at
            ]
        out_ref[:, at] = t_ref[i].astype(BF16)


def shaped(*shape, dtype=F32):
    return jax.ShapeDtypeStruct(shape, dtype)


def activations(
    state_input, decay_real, frequency, log_step, drive_real, drive_imag,
    read_real, read_imag, skip_gain, weights,
):
    rows, chans = state_input.shape
    groups, states = decay_real.shape
    flat = groups * states
    peers = lax.axis_size("sp")
    me = lax.axis_index("sp").reshape(1)
    log_row = log_step.reshape(1, groups)
    b = [part.transpose(0, 2, 1).reshape(chans, states) for part in (drive_real, drive_imag)]
    c = [part.reshape(chans, states) for part in (read_real, read_imag)]
    skip = skip_gain.reshape(1, chans)
    drive_scratch = [
        pltpu.VMEM((chans // LANES, rows, LANES), F32),
        pltpu.VMEM((rows, chans), F32),
        pltpu.VMEM((rows, flat), F32),
        pltpu.VMEM((rows, flat), F32),
    ]
    whole = pl.BlockSpec(memory_space=pltpu.VMEM)
    end, seg, row, weight = pl.pallas_call(
        ends_kernel,
        out_shape=(
            shaped(peers, 2 * flat // LANES, LANES, dtype=BF16),
            shaped(2, SEGMENTS, flat),
            shaped(4, flat),
            shaped(weights[0].shape[0], sum(w.shape[1] for w in weights), dtype=BF16),
        ),
        in_specs=[pl.BlockSpec(memory_space=pltpu.SMEM), *[whole] * 9],
        scratch_shapes=drive_scratch,
        name="ssm_ends",
    )(me, decay_real, frequency, log_row, state_input, *b, *weights)
    weight = lax.all_gather(weight, "sp", axis=0, tiled=True)
    pieces = lax.all_to_all(end, "sp", 0, 0, tiled=True)
    local, power = pl.pallas_call(
        local_kernel,
        out_shape=(shaped(rows, chans), shaped(rows, 2 * flat, dtype=BF16)),
        scratch_shapes=[
            *drive_scratch,
            pltpu.VMEM((rows, 2 * flat), BF16),
            pltpu.VMEM((2, SEGMENTS, flat), F32),
        ],
        cost_estimate=pl.CostEstimate(
            flops=8 * rows * flat * chans, bytes_accessed=8 * rows * flat, transcendentals=0
        ),
        name="ssm_local",
    )(row, seg, state_input, *b, *c, skip)
    acts = pl.pallas_call(
        finish_kernel,
        out_shape=shaped(rows, chans, dtype=BF16),
        scratch_shapes=[pltpu.VMEM((chans // LANES, rows, LANES), F32)],
        name="ssm_finish",
    )(pieces, row, *c, local, power)
    return acts, weight


def ring(array, by):
    peers = lax.axis_size("tp")
    return lax.ppermute(array, "tp", [(i, (i + by) % peers) for i in range(peers)])


def rows_at(array, index, size):
    return lax.dynamic_slice_in_dim(array, index * size, size, 0)


def gathered(top, low):
    left_top = ring(top, 1)
    right_low = ring(low, -1)
    left_low = ring(low, 1)
    right_top = ring(top, -1)
    far_top = ring(left_top, 1)
    far_low = ring(right_low, -1)
    return (left_top, left_low), (right_top, right_low), (far_top, far_low)


def summed(far, right, left, own):
    half = own.shape[0] // 2
    from_left_low = ring(right[half:].astype(BF16), 1)
    from_right_top = ring(left[:half].astype(BF16), -1)
    far = far.astype(BF16)
    passing_up = ring(far[:half], 1)
    passing_down = ring(far[half:], -1)
    from_left_top = ring((right[:half] + passing_up.astype(F32)).astype(BF16), 1)
    from_right_low = ring((left[half:] + passing_down.astype(F32)).astype(BF16), -1)
    top = own[:half] + from_right_top.astype(F32) + from_left_top.astype(F32)
    low = own[half:] + from_left_low.astype(F32) + from_right_low.astype(F32)
    return top, low


def summed_late(far, right, left, own):
    half = own.shape[0] // 2
    far = far.astype(BF16)
    passing_up = ring(far[:half], 1)
    passing_down = ring(far[half:], -1)
    right = right + jnp.pad(passing_up, ((0, half), (0, 0))).astype(F32)
    left = left + jnp.pad(passing_down, ((half, 0), (0, 0))).astype(F32)
    from_left, from_right = ring(right.astype(BF16), 1), ring(left.astype(BF16), -1)
    total = own + from_left.astype(F32) + from_right.astype(F32)
    return total[:half], total[half:]


def shards(
    residual, state_input, gate_input, decay_real, frequency, log_step,
    drive_real, drive_imag, read_real, read_imag, skip_gain,
    value_weight, glu_weight, mix_weight, norm_gain, mlp_gate, mlp_up, mlp_down,
):
    peers, me = lax.axis_size("tp"), lax.axis_index("tp")
    assert peers == 4
    hidden_width = mlp_gate.shape[1]
    chans = state_input.shape[1]
    acts, weight = activations(
        state_input, decay_real, frequency, log_step, drive_real, drive_imag,
        read_real, read_imag, skip_gain, (mlp_gate, mlp_up, mlp_down.T),
    )
    both, down_weight = weight[:, : 2 * hidden_width], weight[:, 2 * hidden_width :]
    places = dict(
        zip((0, 3, 1, 2), (acts, ring(acts, 1), ring(acts, -1), ring(acts, 2)))
    )

    def project(w):
        total = None
        for place, rows in places.items():
            part = jnp.dot(
                rows, rows_at(w, (me + place) % peers, chans), preferred_element_type=F32
            )
            total = part if total is None else total + part
        return total

    value, gated = project(value_weight), project(glu_weight)
    mixed = (jax.nn.sigmoid(gate_input.astype(F32)) * value * jax.nn.sigmoid(gated)).astype(BF16)

    owned = residual.shape[0]

    def mix(place):
        rows = rows_at(mixed, (me + place) % peers, owned)
        return jnp.dot(rows, mix_weight, preferred_element_type=F32)

    far = mix(2)
    branch = summed(far, mix(1), mix(3), mix(0))
    half = owned // 2
    inner, normed = [], []
    for i, part in enumerate(branch):
        inner.append(residual[i * half : (i + 1) * half].astype(F32) + part)
        scale = lax.rsqrt(jnp.mean(inner[i] * inner[i], axis=-1, keepdims=True) + EPSILON)
        normed.append((inner[i] * scale * norm_gain).astype(BF16))
    left, right, far = gathered(*normed)

    def feed(rows):
        hidden = jnp.dot(rows, both, preferred_element_type=F32)
        hidden = (jax.nn.silu(hidden[:, :hidden_width]) * hidden[:, hidden_width:]).astype(BF16)
        return lax.dot_general(hidden, down_weight, NT, preferred_element_type=F32)

    sides = feed(jnp.concatenate([*left, *right], axis=0))
    far = feed(jnp.concatenate(far, axis=0))
    own = feed(jnp.concatenate(normed, axis=0))
    down = summed_late(far, sides[owned:], sides[:owned], own)
    return jnp.concatenate(
        [(i + 0.5 * part).astype(BF16) for i, part in zip(inner, down)], axis=0
    )


def solution(mesh):
    placed = (
        P(("grp", "sp", "tp"), None),
        P(("grp", "sp"), "tp"),
        P(("grp", "sp"), "tp"),
        P("tp", None),
        P("tp", None),
        P("tp"),
        P("tp", None, None),
        P("tp", None, None),
        P("tp", None, None),
        P("tp", None, None),
        P("tp"),
        P(None, "tp"),
        P(None, "tp"),
        P("tp", None),
        P(),
        P("sp", "tp"),
        P("sp", "tp"),
        P("tp", "sp"),
    )

    return jax.shard_map(
        shards, mesh=mesh, in_specs=placed, out_specs=P(("grp", "sp", "tp"), None), check_vma=False
    )
```
